256 devices in a mesh: ep: 128 (over z, y, x), tp: 2 (over core).
Axes of the slice: x: 4, y: 4, z: 8, core: 2. Of those that a mesh axis runs over, the one named last changes fastest.
Arguments:
- tokens: bfloat16 [2048, 2048], P('ep', 'tp'), may hold values from -6 to 6
- state: float32 [2048, 4, 128, 128], P('ep', 'tp'), may hold values from -4 to 4
- norm_mix: float32 [2048], replicated, may hold values from 0.1 to 1.9
- w_query: bfloat16 [2048, 512], P(None, 'tp'), may hold values from -0.125 to 0.125
- w_key: bfloat16 [2048, 512], P(None, 'tp'), may hold values from -0.125 to 0.125
- w_value: bfloat16 [2048, 512], P(None, 'tp'), may hold values from -0.125 to 0.125
- w_out: bfloat16 [512, 2048], P('tp'), may hold values from -0.25 to 0.25
- norm_ffn: float32 [2048], P('tp'), may hold values from 0.1 to 1.9
- gate_vector: bfloat16 [2048], P('tp'), may hold values from -0.125 to 0.125
- dense_gate: bfloat16 [2048, 2816], P('tp', 'ep'), may hold values from -0.125 to 0.125
- dense_up: bfloat16 [2048, 2816], P('tp', 'ep'), may hold values from -0.125 to 0.125
- dense_down: bfloat16 [2816, 2048], P('ep', 'tp'), may hold values from -0.109375 to 0.109375
- exp_gate: bfloat16 [128, 2048, 176], P('ep', None, 'tp'), may hold values from -0.125 to 0.125
- exp_up: bfloat16 [128, 2048, 176], P('ep', None, 'tp'), may hold values from -0.125 to 0.125
- exp_down: bfloat16 [128, 176, 2048], P('ep', 'tp'), may hold values from -0.109375 to 0.109375
- routes: int32 [2048, 2], P('ep'), may hold values from 0 to 7, all different within a row; in each aligned block of 16 rows (0 to 15, 16 to 31, ...) at most 5 rows name the same one
- route_w: bfloat16 [2048, 2], P('ep'), may hold values from 0.099609375 to 1
Outputs:
- mixed: bfloat16 [2048, 2048], P('ep', 'tp')
- new_state: float32 [2048, 4, 128, 128], P('ep', 'tp')
The draws below stay inside these ranges and needn't reach their ends.
Inputs may be any that keep to these rules, and one draw needn't show every extreme that they name: `routes`: each row names 2 different experts. Within the rows of one device (aligned blocks of 16 rows) no expert is named by more than 5 rows, a bound that some blocks reach.
All inputs are finite; a program needn't handle non-finite values.
Results may differ from the reference program's by a relative error of at most 0.014.
Values may be sent and summed in bfloat16 or wider, within the bound.
A program may use at most 128 MiB of HBM per device.

```python
import math
import jax
import jax.numpy as jnp
import numpy as np
from jax import lax

D = 2048
HEADS = 4
HEAD = 128
FF = 2816
FF_D = 2816
EXPERTS = 8
TOPK = 2
SEQ_DEV = 16
CAP = 5
E_SPLIT = 16
TOKENS = 2048
N_EP = 128
N_TP = 2


def levels(own_key, shape, pieces, low, largest):
    level = 1.0
    for dim, blocks in pieces:
        draws = jax.random.uniform(jax.random.fold_in(jax.random.fold_in(own_key, 6), dim), (blocks,), jnp.float32, low / len(pieces), largest / len(pieces))
        level = level * jnp.repeat(jnp.exp(draws), shape[dim] // blocks).reshape((-1,) + (1,) * (len(shape) - 1 - dim))
    return level


def shared_out(own_key, own, number, rows, count, top, reach, lean):
    order = jax.random.permutation(own_key, count)
    packed, usual = shares(count, rows * top, reach, lean, True), shares(count, rows * top, reach, lean, False)
    places = jnp.arange(count)

    def named(lengths, turn):
        used = int((lengths > 0).sum())
        fixed = max(1, used // 4)
        moved = fixed + (places - fixed + turn * (used - fixed)) % max(1, count - fixed)
        return jnp.zeros((count,), jnp.int32).at[order[jnp.where(places < fixed, places, moved)]].set(jnp.asarray(lengths, jnp.int32))

    lengths = jnp.where(number % 4 == 0, named(packed, number // 4), named(usual, number - number // 4 - 1))
    mixed = jax.random.permutation(jax.random.fold_in(own, 3), count)
    donor, taker = mixed[0:count // 2 * 2:2], mixed[1:count // 2 * 2:2]
    slack = jnp.minimum(lengths[donor] - 1, reach - lengths[taker]) // 2
    slack = jnp.where((donor == order[0]) | (taker == order[0]) | (lengths[taker] == 0), 0, jnp.maximum(slack, 0))
    moved = jax.random.randint(jax.random.fold_in(own, 4), (count // 2,), 0, 1 << 20) % (slack + 1)
    lengths = lengths.at[donor].add(-moved).at[taker].add(moved)
    labels = jnp.searchsorted(jnp.cumsum(lengths), jnp.arange(rows * top), side="right").astype(jnp.int32)
    listing = labels.reshape(top, rows).T
    listing = listing[jax.random.permutation(jax.random.fold_in(own, 1), rows)]
    turn = jax.random.randint(jax.random.fold_in(own, 2), (rows, 1), 0, top)
    return jnp.take_along_axis(listing, (jnp.arange(top)[None, :] + turn) % top, axis=1)


def shares(number_of, total, bound, slope, full):
    loads = [(1 << 20) // math.isqrt(grade ** slope) + 1 for grade in range(1, number_of + 1)]
    largest = bound if full else min(bound, max(-(-total // number_of), total * loads[0] // sum(loads)))
    least = 1 if total - largest >= number_of - 1 else 0
    counts, spare = [largest] + [least] * (number_of - 1), total - largest - least * (number_of - 1)
    while spare > 0:
        free = [i for i in range(1, number_of) if counts[i] < largest] or [i for i in range(1, number_of) if counts[i] < bound]
        whole, left = sum([loads[i] for i in free]), spare
        for i in free:
            extra = min(bound - counts[i], max(1, left * loads[i] // whole), spare)
            counts[i] = counts[i] + extra
            spare = spare - extra
    return np.array(counts)


def gaussian(own_key, dims, scale, bound, cuts=(), kind=jnp.bfloat16):
    level = levels(own_key, dims, cuts, -0.22, 0.18) if cuts else 1.0
    entries = jax.random.normal(own_key, dims, jnp.float32) * scale * level
    return jnp.minimum(jnp.maximum(entries, -bound), bound).astype(kind)


def setup_inputs(seed: int = 0) -> dict:
    seeds = jax.random.split(jax.random.key(seed), 18)
    tokens = gaussian(seeds[0], (TOKENS, D), 1.0, 6.0, ((0, 128), (1, 2)))
    state = gaussian(seeds[1], (TOKENS, HEADS, HEAD, HEAD), 0.5, 4.0, ((0, 128), (1, 2)), jnp.float32)
    norm_mix = jnp.clip(1.0 + 0.18 * jax.random.normal(seeds[2], (D,), jnp.float32), 0.1, 1.9)
    w_query = gaussian(seeds[3], (D, HEADS * HEAD), D ** -0.5, 0.125, ((1, 2),))
    w_key = gaussian(seeds[4], (D, HEADS * HEAD), D ** -0.5, 0.125, ((1, 2),))
    w_value = gaussian(seeds[5], (D, HEADS * HEAD), D ** -0.5, 0.125, ((1, 2),))
    w_out = gaussian(seeds[6], (HEADS * HEAD, D), (HEADS * HEAD) ** -0.5, 0.25, ((0, 2),))
    norm_ffn = jnp.clip(1.0 + 0.18 * jax.random.normal(seeds[7], (D,), jnp.float32), 0.1, 1.9)
    gate_vector = gaussian(seeds[8], (D,), D ** -0.5, 0.125, ((0, 2),))
    dense_gate = gaussian(seeds[9], (D, FF_D), D ** -0.5, 0.125, ((0, 2), (1, 128)))
    dense_up = gaussian(seeds[10], (D, FF_D), D ** -0.5, 0.125, ((0, 2), (1, 128)))
    dense_down = gaussian(seeds[11], (FF_D, D), FF_D ** -0.5, 0.109375, ((0, 128), (1, 2)))
    exp_gate = gaussian(seeds[12], (EXPERTS * E_SPLIT, D, FF // E_SPLIT), D ** -0.5, 0.125, ((0, 128), (2, 2)))
    exp_up = gaussian(seeds[13], (EXPERTS * E_SPLIT, D, FF // E_SPLIT), D ** -0.5, 0.125, ((0, 128), (2, 2)))
    exp_down = gaussian(seeds[14], (EXPERTS * E_SPLIT, FF // E_SPLIT, D), FF ** -0.5, 0.109375, ((0, 128), (1, 2)))
    routes_keys = jax.random.split(jax.random.fold_in(seeds[15], 1), TOKENS // SEQ_DEV)
    routes_turns = jax.random.permutation(jax.random.fold_in(seeds[15], 3), TOKENS // SEQ_DEV)
    routes = jax.vmap(lambda own, number: shared_out(jax.random.fold_in(seeds[15], 2), own, number, SEQ_DEV, EXPERTS, TOPK, CAP, 1))(routes_keys, routes_turns).reshape((TOKENS, TOPK))
    route_w = jnp.clip(0.099609375 + 0.9003906 * jax.random.uniform(seeds[16], (TOKENS, TOPK), jnp.float32) ** levels(seeds[16], (TOKENS, TOPK), ((0, 128),), -0.2, 0.2), 0.099609375, 1.0).astype(jnp.bfloat16)
    return dict(tokens=tokens, state=state, norm_mix=norm_mix, w_query=w_query, w_key=w_key, w_value=w_value, w_out=w_out, norm_ffn=norm_ffn, gate_vector=gate_vector, dense_gate=dense_gate, dense_up=dense_up, dense_down=dense_down, exp_gate=exp_gate, exp_up=exp_up, exp_down=exp_down, routes=routes, route_w=route_w)


epsilon = 1e-06

def reference(tokens, state, norm_mix, w_query, w_key, w_value, w_out, norm_ffn, gate_vector, dense_gate, dense_up, dense_down, exp_gate, exp_up, exp_down, routes, route_w):
    highest = lax.Precision.HIGHEST
    tok_f = tokens.astype(jnp.float32)
    normed = (tok_f * lax.rsqrt(lax.optimization_barrier(jnp.mean(tok_f * tok_f, axis=1, keepdims=True)) + epsilon) * norm_mix).astype(jnp.bfloat16)
    query = jnp.dot(normed, w_query, preferred_element_type=jnp.float32).astype(jnp.bfloat16)
    key_rows = jnp.dot(normed, w_key, preferred_element_type=jnp.float32).astype(jnp.bfloat16)
    value_rows = jnp.dot(normed, w_value, preferred_element_type=jnp.float32).astype(jnp.bfloat16)
    row_count = tokens.shape[0]
    query3 = query.astype(jnp.float32).reshape(row_count, HEADS, HEAD)
    key3 = key_rows.astype(jnp.float32).reshape(row_count, HEADS, HEAD) * HEAD ** (-0.5)
    value3 = value_rows.astype(jnp.float32).reshape(row_count, HEADS, HEAD)
    head_ids = jnp.arange(HEADS, dtype=jnp.float32)
    decay = 1.0 - jnp.exp2(-3.0 - 2.0 * head_ids)
    new_state = decay[None, :, None, None] * state + jnp.einsum('shd,she->shde', key3, value3, precision=highest)
    read = jnp.einsum('shd,shde->she', query3, new_state, precision=highest)
    centre = lax.optimization_barrier(jnp.mean(read, axis=2, keepdims=True))
    spread = lax.optimization_barrier(jnp.mean(jnp.square(read - centre), axis=2, keepdims=True))
    heads_out = ((read - centre) * lax.rsqrt(spread + epsilon)).astype(jnp.bfloat16).reshape(row_count, HEADS * HEAD)
    group_cols = HEADS * HEAD // N_TP
    mix_sum = jnp.zeros((row_count, D), jnp.float32)
    for group in range(N_TP):
        lower = group * group_cols
        partial_value = jnp.dot(heads_out[:, lower:lower + group_cols], w_out[lower:lower + group_cols], preferred_element_type=jnp.float32)
        rounded = lax.optimization_barrier(partial_value.astype(jnp.bfloat16))
        mix_sum = mix_sum + rounded.astype(jnp.float32)
    after = (tok_f + mix_sum).astype(jnp.bfloat16)
    after_f = after.astype(jnp.float32)
    normed2 = (after_f * lax.rsqrt(lax.optimization_barrier(jnp.mean(after_f * after_f, axis=1, keepdims=True)) + epsilon) * norm_ffn).astype(jnp.bfloat16)
    dense_pre = jnp.dot(normed2, dense_gate, preferred_element_type=jnp.float32)
    up_pre = jnp.dot(normed2, dense_up, preferred_element_type=jnp.float32)
    logit = jnp.dot(normed2, gate_vector, preferred_element_type=jnp.float32)
    dense_hidden = (jax.nn.sigmoid(logit)[:, None] * jax.nn.silu(dense_pre) * up_pre).astype(jnp.bfloat16)
    dense = jnp.dot(dense_hidden, dense_down, preferred_element_type=jnp.float32)
    group_size = N_EP // EXPERTS
    part_ff = exp_gate.shape[2]
    gate_all = exp_gate.reshape(EXPERTS, group_size, D, part_ff).transpose(0, 2, 1, 3).reshape(EXPERTS, D, group_size * part_ff)
    up_all = exp_up.reshape(EXPERTS, group_size, D, part_ff).transpose(0, 2, 1, 3).reshape(EXPERTS, D, group_size * part_ff)
    down_all = exp_down.reshape(EXPERTS, group_size * part_ff, D)
    onehot = (routes[:, :, None] == jnp.arange(EXPERTS, dtype=jnp.int32)[None, None, :]).astype(jnp.float32)
    member = lax.optimization_barrier(jnp.sum(onehot, axis=1))
    weight = lax.optimization_barrier(jnp.sum(onehot * route_w.astype(jnp.float32)[:, :, None], axis=1))
    member_b = member.reshape(N_EP, SEQ_DEV, EXPERTS)
    slot_b = jnp.cumsum(member_b, axis=1) - member_b
    weight_b = weight.reshape(N_EP, SEQ_DEV, EXPERTS)
    rows_b = normed2.astype(jnp.float32).reshape(N_EP, SEQ_DEV, D)
    slot_ids = jnp.arange(CAP, dtype=jnp.float32)

    def one_expert(total, inputs):
        gate_w, up_w, down_w, pick, place, scale = inputs
        select = pick[:, None, :] * (place[:, None, :] == slot_ids[None, :, None]).astype(jnp.float32)
        chosen = jnp.einsum('ncr,nrd->ncd', select, rows_b, precision=highest).astype(jnp.bfloat16).reshape(N_EP * CAP, D)
        gate_pre = jnp.dot(chosen, gate_w, preferred_element_type=jnp.float32)
        up_part = jnp.dot(chosen, up_w, preferred_element_type=jnp.float32)
        hidden = (jax.nn.silu(gate_pre) * up_part).astype(jnp.bfloat16)
        result = jnp.dot(hidden, down_w, preferred_element_type=jnp.float32).reshape(N_EP, CAP, D)
        contrib = jnp.einsum('ncr,ncd->nrd', select * scale[:, None, :], result, precision=highest)
        return (total + contrib, None)
    moe, _ = lax.scan(one_expert, jnp.zeros((N_EP, SEQ_DEV, D), jnp.float32), (gate_all, up_all, down_all, member_b.transpose(2, 0, 1), slot_b.transpose(2, 0, 1), weight_b.transpose(2, 0, 1)))
    mixed = (after_f + moe.reshape(row_count, D) + dense).astype(jnp.bfloat16)
    return (mixed, new_state)
```

```python
import functools

import jax
import jax.numpy as jnp
from jax import lax
from jax.experimental import pallas as pl
from jax.experimental.pallas import tpu as pltpu
from jax.sharding import PartitionSpec as P

EXPERTS = 8
CAP = 5
SLOT = 8
SIDE = 4
PLANE = SIDE * SIDE
TRIPS = ((0, 1, 7), (2, 6, 3), (5, 4))
epsilon = 1e-06
MESH = pl.DeviceIdType.MESH
F32 = jnp.float32
BF16 = jnp.bfloat16


def dot(a, b):
    return jnp.dot(a, b, preferred_element_type=F32)


def dot_t(a, b):
    return lax.dot_general(a, b, (((1,), (1,)), ((), ())), preferred_element_type=F32)


def silu(v):
    return v / (1.0 + jnp.exp(-v))


def iota(shape, dim):
    return lax.broadcasted_iota(jnp.int32, shape, dim)


def kernel(
    tokens_h,
    norm_mix_h,
    routes_h,
    route_w_h,
    norm_ffn_h,
    gate_vec_h,
    state,
    w_query,
    w_key,
    w_value,
    w_out,
    dense_gate,
    dense_up,
    dense_down,
    exp_gate,
    exp_up,
    exp_down,
    mixed,
    ns,
    tokens,
    norm_mix,
    routes,
    route_w,
    norm_ffn,
    gate_vec,
    tok_p,
    wq,
    wk,
    wv,
    wo_o,
    wo_p,
    eg,
    eu,
    ed,
    st,
    ho_o,
    ho_p,
    sel_m,
    comb_m,
    lg_s,
    lg_r,
    wbuf,
    wdg,
    wdu,
    wdd,
    w1,
    w2,
    xs,
    zr,
    xz,
    xe,
    pe_o,
    pe_s,
    pe_r,
    pd_o,
    pd_s,
    pd_r,
    y32,
    yb,
    rb,
    rd,
    rs,
    rf,
    sa,
    sb,
    ab,
    ad,
    ax,
    af,
    zs,
    zret,
    yz0,
    yzs,
    yzr,
    lsem,
    ssem,
    rsem,
):
    R, H = tokens.shape
    D = 2 * H
    heads, hs = state.shape[1], state.shape[2]
    HW = heads * hs
    FE = eg.shape[1]
    FD = wbuf.shape[2]
    Z = EXPERTS
    me = lax.axis_index("ep")
    tp = lax.axis_index("tp")
    other = 1 - tp
    z, y_at, x_at = me // PLANE, (me // SIDE) % SIDE, me % SIDE

    def in_plane(dy, dx):
        return {
            "ep": z * PLANE + ((y_at + dy + SIDE) % SIDE) * SIDE + (x_at + dx + SIDE) % SIDE,
            "tp": tp,
        }

    first = {d: in_plane(tp * d, other * d) for d in (1, -1)}
    second = {d: in_plane(other * d, tp * d) for d in (1, -1)}
    zpeer = [{"ep": ((z + i) % Z) * PLANE + me % PLANE, "tp": tp} for i in range(Z)]
    partner = {"ep": me, "tp": other}

    def place(p):
        turned = (p % SIDE) * SIDE + p // SIDE
        return p + tp * (turned - p)

    own = pl.ds(pl.multiple_of(tp * H, H), H)
    oth = pl.ds(pl.multiple_of(other * H, H), H)

    sent = []

    def remote(src, dst, dev):
        k = len(sent)
        copy = pltpu.make_async_remote_copy(
            src_ref=src,
            dst_ref=dst,
            send_sem=ssem.at[k],
            recv_sem=rsem.at[k],
            device_id=dev,
            device_id_type=MESH,
        )
        copy.start()
        sent.append(copy)
        return copy

    local = {}

    def load(name, src, dst):
        copy = pltpu.make_async_copy(src, dst, lsem.at[len(local)])
        copy.start()
        local[name] = copy

    class Gather:
        def __init__(self, buf, via):
            self.buf, self.via = buf, via
            self.up, self.down = {}, {}

        def spread(self, a):
            at = self.buf.at
            self.up[a] = remote(at[a], at[3 * SIDE + a], second[1])
            self.down[a] = remote(at[a], at[SIDE + a], second[-1])

        def start(self):
            at = self.buf.at
            self.f_up = remote(at[0], at[3], first[1])
            self.f_down = remote(at[0], at[1], first[-1])
            self.spread(0)

        def one(self):
            at = self.buf.at
            self.f_up.wait_recv()
            if self.via > 0:
                self.f_two = remote(at[3], at[2], first[1])
            self.spread(3)
            self.f_down.wait_recv()
            if self.via < 0:
                self.f_two = remote(at[1], at[2], first[-1])
            self.spread(1)

        def two(self):
            self.f_two.wait_recv()
            self.spread(2)

        def relay(self, todo):
            at = self.buf.at
            for a in todo:
                self.up[a].wait_recv()
                if a in (0, 1):
                    self.up[a + SIDE] = remote(at[3 * SIDE + a], at[2 * SIDE + a], second[1])
                self.down[a].wait_recv()
                if a in (2, 3):
                    self.up[a + SIDE] = remote(at[SIDE + a], at[2 * SIDE + a], second[-1])

        def finish(self):
            for a in range(SIDE):
                self.up[a + SIDE].wait_recv()

    small = (
        (tokens_h, tokens),
        (norm_mix_h, norm_mix),
        (routes_h, routes),
        (route_w_h, route_w),
        (norm_ffn_h, norm_ffn),
        (gate_vec_h, gate_vec),
    )
    barrier = pltpu.get_barrier_semaphore()
    greeted = [partner, first[1], first[-1], second[1], second[-1]] + zpeer[1:]
    for dev in greeted:
        pl.semaphore_signal(barrier, inc=1, device_id=dev, device_id_type=MESH)

    for t, (src, dst) in enumerate(small):
        load(f"s{t}", src, dst)
    for t, src in enumerate((dense_gate, dense_up, dense_down)):
        load(f"d{t}", src, wbuf.at[0, t])
    for t, (src, dst) in enumerate(((w_query, wq), (w_key, wk), (w_value, wv))):
        load(f"p{t}o", src.at[own, :], dst.at[0])
        load(f"p{t}p", src.at[oth, :], dst.at[1])
    load("st", state, st)
    load("wo0", w_out.at[:, own], wo_o.at[0])
    load("wo1", w_out.at[:, oth], wo_o.at[1])
    load("eg", exp_gate.at[:, own], eg.at[tp])
    load("eu", exp_up.at[:, own], eu.at[tp])
    load("ed", exp_down.at[0, :, own], ed.at[tp])

    for t in (2, 3):
        local[f"s{t}"].wait()
    row_id = iota((EXPERTS, R), 0)
    wt = jnp.zeros((EXPERTS, R), F32)
    member = jnp.zeros((EXPERTS, R), F32)
    named = routes[...]
    gains = route_w[...].astype(F32)
    for t in range(routes.shape[0]):
        hit = row_id == named[t : t + 1, :]
        wt = wt + jnp.where(hit, gains[t : t + 1, :], 0.0)
        member = member + jnp.where(hit, 1.0, 0.0)
    blank = jnp.zeros((EXPERTS, 128 - R), F32)
    wt = jnp.concatenate([wt, blank], axis=1)
    member = jnp.concatenate([member, blank], axis=1)
    before = jnp.where(iota((128, 128), 0) < iota((128, 128), 1), 1.0, 0.0).astype(BF16)
    rank = dot(member.astype(BF16), before)
    slot_id = iota((SLOT, 128), 0).astype(F32)
    picks, scaled = [], []
    for e in range(EXPERTS):
        pick = jnp.where(rank[e : e + 1] == slot_id, member[e : e + 1], 0.0)
        picks.append(pick)
        scaled.append(pick * wt[e : e + 1])
    sel_m[...] = jnp.concatenate(picks, axis=0)
    scaled.append(jnp.zeros((128 - EXPERTS * SLOT, 128), F32))
    comb_m[...] = jnp.concatenate(scaled, axis=0).T[:R]

    for t in (0, 1, 4, 5):
        local[f"s{t}"].wait()
    for t in range(3):
        local[f"d{t}"].wait()
    pl.semaphore_wait(barrier, len(greeted))

    c_tok = remote(tokens, tok_p, partner)
    weights = Gather(wbuf, 1)
    weights.start()
    c_wo0 = remote(w_out.at[:, oth], wo_p.at[0], partner)
    c_wo1 = remote(w_out.at[:, own], wo_p.at[1], partner)
    c_eg = remote(exp_gate.at[:, oth], eg.at[tp], partner)
    c_eu = remote(exp_up.at[:, oth], eu.at[tp], partner)
    c_ed = remote(exp_down.at[0, :, oth], ed.at[tp], partner)

    tok_f = tokens[...].astype(F32)
    c_tok.wait_recv()
    tok_pf = tok_p[...].astype(F32)
    total = jnp.sum(tok_f * tok_f, axis=1, keepdims=True) + jnp.sum(
        tok_pf * tok_pf, axis=1, keepdims=True
    )
    scale = lax.rsqrt(total / D + epsilon)
    gain_o = norm_mix[:, own]
    gain_p = norm_mix[:, oth]
    nx_o = (tok_f * scale * gain_o).astype(BF16)
    nx_p = (tok_pf * scale * gain_p).astype(BF16)
    proj = []
    for t, w in enumerate((wq, wk, wv)):
        local[f"p{t}o"].wait()
        part = dot(nx_o, w[0])
        local[f"p{t}p"].wait()
        proj.append((part + dot(nx_p, w[1])).astype(BF16).astype(F32))
    q, k, v = proj
    k = k * hs ** (-0.5)
    pad = jnp.zeros((128 - R, HW), F32)
    q_t = jnp.concatenate([q, pad], axis=0).T
    k_t = jnp.concatenate([k, pad], axis=0).T
    head_id = tp * heads
    local["st"].wait()
    decays = []
    for h in range(heads):
        cols = slice(h * hs, (h + 1) * hs)
        idv = jnp.zeros((1, 128), F32) + (head_id + h).astype(F32)
        decay = 1.0 - jnp.exp2(-3.0 - 2.0 * idv)
        decays.append(decay)
        rows = []
        for s in range(R):
            rows.append(jnp.sum(st[s, h] * q_t[cols, s : s + 1], axis=0, keepdims=True))
        qs = jnp.concatenate(rows, axis=0)
        qk = jnp.sum(q[:, cols] * k[:, cols], axis=1, keepdims=True)
        read = decay * qs + qk * v[:, cols]
        centre = jnp.mean(read, axis=1, keepdims=True)
        dev = read - centre
        spread = jnp.mean(dev * dev, axis=1, keepdims=True)
        ho_o[:, cols] = (dev * lax.rsqrt(spread + epsilon)).astype(BF16)
    c_ho = remote(ho_o, ho_p, partner)
    weights.one()
    ho = ho_o[...]
    local["wo0"].wait()
    local["wo1"].wait()
    a_o = dot(ho, wo_o[0]).astype(BF16).astype(F32)
    a_p = dot(ho, wo_o[1]).astype(BF16).astype(F32)
    c_wo0.wait_recv()
    c_wo1.wait_recv()
    c_ho.wait_recv()
    hp = ho_p[...]
    a_o = a_o + dot(hp, wo_p[0]).astype(BF16).astype(F32)
    a_p = a_p + dot(hp, wo_p[1]).astype(BF16).astype(F32)
    after = (tok_f + a_o).astype(BF16).astype(F32)
    after_p = (tok_pf + a_p).astype(BF16).astype(F32)
    squares = jnp.sum(after * after, axis=1, keepdims=True) + jnp.sum(
        after_p * after_p, axis=1, keepdims=True
    )
    normed = (after * lax.rsqrt(squares / D + epsilon) * norm_ffn[...]).astype(BF16)

    chosen = dot(sel_m[:, :R].astype(BF16), normed).astype(BF16)
    xs[...] = chosen.astype(F32).reshape(EXPERTS, SLOT, H).astype(BF16)
    xz[0] = normed
    c_zr = {}
    for trip in TRIPS:
        for i in trip:
            if i:
                c_zr[i] = remote(xs.at[(z + i) % Z], zr.at[Z - i], zpeer[i])
    c_xz = {}
    for i in (1, 7, 2, 6, 3, 5, 4):
        c_xz[i] = remote(xz.at[0], xz.at[Z - i], zpeer[i])
    gate_row = gate_vec[...].astype(F32)
    gate_row = jnp.concatenate([gate_row[r : r + 1] for r in range(H // 128)], axis=1)
    logit = jnp.sum(normed.astype(F32) * gate_row, axis=1, keepdims=True)
    lg_s[...] = logit + jnp.zeros((R, 128), F32)
    c_lg = remote(lg_s, lg_r, partner)
    weights.two()
    weights.relay((0,))

    def new_state(h):
        cols = slice(h * hs, (h + 1) * hs)
        for s in range(R):
            ns[s, h] = decays[h] * st[s, h] + k_t[cols, s : s + 1] * v[s : s + 1, cols]

    new_state(0)

    chunks = [Gather(xe.at[c], 1 if c % 2 == 0 else -1) for c in range(len(TRIPS))]

    def pack(c):
        parts = []
        for i in TRIPS[c]:
            if i == 0:
                parts.append(xs[z].astype(F32))
            else:
                c_zr[Z - i].wait_recv()
                parts.append(zr[i].astype(F32))
        parts.append(jnp.zeros((32 - SLOT * len(parts), H), F32))
        rows = jnp.concatenate(parts, axis=0).astype(BF16)
        r, s = iota((R, 32), 0), iota((R, 32), 1)
        take = jnp.zeros((R, 32), F32)
        for j in range(len(TRIPS[c])):
            hit = (s - SLOT * j == r - CAP * j) & (r >= CAP * j) & (r < CAP * (j + 1))
            take = take + jnp.where(hit, 1.0, 0.0)
        xe[c, 0] = dot(take.astype(BF16), rows).astype(BF16)
        chunks[c].start()

    pack(0)
    weights.relay((3, 1))
    new_state(1)
    pack(1)
    chunks[0].one()
    pack(2)
    weights.relay((2,))

    for name in ("eg", "eu", "ed"):
        local[name].wait()
    for copy in (c_eg, c_eu, c_ed):
        copy.wait_recv()
    for t in range(2):
        for src, dst in ((eg, w1.at[0, t]), (eu, w1.at[1, t]), (ed, w2.at[t])):
            dst[:FE] = src[t]
            dst[FE:] = jnp.zeros((128 - FE, H), BF16)

    chunks[0].two()
    chunks[1].one()
    chunks[0].relay((0, 3))
    chunks[2].one()
    chunks[1].two()
    chunks[0].relay((1, 2))
    chunks[2].two()
    chunks[1].relay((0, 3, 1, 2))

    c_pe = {}

    def before_act(c):
        chunks[c].finish()
        x = jnp.concatenate([xe[c, place(p)] for p in range(PLANE)], axis=0)
        pre = dot_t(x, w1[...].reshape(4 * 128, H))
        pe_o[c] = pre
        pe_s[c] = pre.astype(BF16)
        c_pe[c] = remote(pe_s.at[c], pe_r.at[c], partner)

    def act(c):
        c_pe[c].wait_recv()
        pre = pe_o[c] + pe_r[c].astype(F32)
        hidden = (silu(pre[:, :256]) * pre[:, 256:]).astype(BF16)
        y = dot(hidden, w2[...].reshape(256, H))
        for p in range(PLANE):
            part = y[p * R : (p + 1) * R]
            y32[c, place(p)] = part
            yb[c, place(p)] = part.astype(BF16)
        at = yb.at
        low, high = lambda b: pl.ds(SIDE * b, 2), lambda b: pl.ds(SIDE * b + 2, 2)
        c_rb[c] = (
            remote(at[c, low(2)], rb.at[c, 0], second[1]),
            remote(at[c, high(2)], rb.at[c, 1], second[-1]),
        )
        c_rd[c] = (
            remote(at[c, high(1)], rd.at[c, 0], second[1]),
            remote(at[c, low(3)], rd.at[c, 1], second[-1]),
        )

    c_rb, c_rd, c_rf, c_ab, c_ad, c_af = {}, {}, {}, {}, {}, {}

    def sum_relay(c):
        c_rb[c][0].wait_recv()
        rs[c, 0] = (y32[c, SIDE : SIDE + 2] + rb[c, 0].astype(F32)).astype(BF16)
        up = remote(rs.at[c, 0], rf.at[c, 0], second[1])
        c_rb[c][1].wait_recv()
        rs[c, 1] = (y32[c, 3 * SIDE + 2 : 4 * SIDE] + rb[c, 1].astype(F32)).astype(BF16)
        c_rf[c] = (up, remote(rs.at[c, 1], rf.at[c, 1], second[-1]))

    def sum_second(c):
        via = chunks[c].via
        near, far = (1, 3) if via > 0 else (3, 1)
        c_rd[c][1].wait_recv()
        c_rf[c][0].wait_recv()
        low = y32[c, 0:2] + rf[c, 0].astype(F32) + rd[c, 1].astype(F32)
        c_rd[c][0].wait_recv()
        c_rf[c][1].wait_recv()
        high = y32[c, 2:4] + rf[c, 1].astype(F32) + rd[c, 0].astype(F32)
        total = (low[0], low[1], high[0], high[1])
        sb[c, 0] = total[2].astype(BF16)
        c_ab[c] = remote(sb.at[c, 0], ab.at[c], first[via])
        sb[c, 1] = total[far].astype(BF16)
        c_ad[c] = remote(sb.at[c, 1], ad.at[c], first[-via])
        sa[c, 0] = total[0]
        sa[c, 1] = total[near]

    def sum_two(c):
        c_ab[c].wait_recv()
        ax[c] = (sa[c, 1] + ab[c].astype(F32)).astype(BF16)
        c_af[c] = remote(ax.at[c], af.at[c], first[chunks[c].via])

    c_ret = {}

    def give_back(c):
        c_ad[c].wait_recv()
        c_af[c].wait_recv()
        total = (sa[c, 0] + ad[c].astype(F32) + af[c].astype(F32)).astype(BF16)
        n = len(TRIPS[c])
        s, r = iota((32, R), 0), iota((32, R), 1)
        put = jnp.zeros((32, R), F32)
        for j in range(n):
            hit = (s - SLOT * j == r - CAP * j) & (r >= CAP * j) & (r < CAP * (j + 1))
            put = put + jnp.where(hit, 1.0, 0.0)
        rows = dot(put.astype(BF16), total)
        for j, i in enumerate(TRIPS[c]):
            block = rows[j * SLOT : (j + 1) * SLOT].astype(BF16)
            if i == 0:
                zret[z] = block
            else:
                zs[i] = block
                c_ret[i] = remote(zs.at[i], zret.at[z], zpeer[i])

    before_act(0)
    chunks[2].relay((0, 3, 1, 2))
    before_act(1)
    act(0)
    weights.finish()
    before_act(2)
    act(1)
    sum_relay(0)

    for p in range(PLANE):
        for t, dst in enumerate((wdg, wdu, wdd)):
            dst[p, :FD] = wbuf[place(p), t]
            dst[p, FD:] = jnp.zeros((32 - FD, H), BF16)
    act(2)
    sum_second(0)
    sum_relay(1)
    for i in range(1, Z):
        c_xz[i].wait_recv()
    x = xz[...].reshape(Z * R, H)
    for t, w in enumerate((wdg, wdu)):
        pre = dot_t(x, w[...].reshape(PLANE * 32, H))
        pd_o[t] = pre
        pd_s[t] = pre.astype(BF16)
    c_pd = remote(pd_s, pd_r, partner)
    sum_two(0)
    sum_second(1)
    sum_relay(2)
    c_pd.wait_recv()
    gate = pd_o[0] + pd_r[0].astype(F32)
    up = pd_o[1] + pd_r[1].astype(F32)
    y = dot((silu(gate) * up).astype(BF16), wdd[...].reshape(PLANE * 32, H))
    yz0[...] = y[:R]
    yzs[...] = y.astype(BF16).reshape(Z, R, H)
    give_back(0)
    c_yz = {}
    for i in range(1, Z):
        c_yz[i] = remote(yzs.at[i], yzr.at[Z - i], zpeer[i])
    sum_two(1)
    sum_second(2)
    give_back(1)
    sum_two(2)
    give_back(2)

    c_lg.wait_recv()
    open_ = 1.0 / (1.0 + jnp.exp(-(lg_s[:, :1] + lg_r[:, :1])))
    dense = yz0[...]
    for i in range(1, Z):
        c_yz[i].wait_recv()
        dense = dense + yzr[Z - i].astype(F32)
    for i in range(1, Z):
        c_ret[i].wait_recv()
    back = zret[...].astype(F32).reshape(EXPERTS * SLOT, H).astype(BF16)
    moe = dot(comb_m[:, : EXPERTS * SLOT].astype(BF16), back)
    mixed[...] = (after + moe + open_ * dense).astype(BF16)
    for copy in sent:
        copy.wait_send()


def store(a_in, b_in, a_out, b_out, sems):
    first = pltpu.make_async_copy(b_in, b_out, sems.at[0])
    second = pltpu.make_async_copy(a_in, a_out, sems.at[1])
    first.start()
    second.start()
    first.wait()
    second.wait()


def body(
    tokens,
    state,
    norm_mix,
    w_query,
    w_key,
    w_value,
    w_out,
    norm_ffn,
    gate_vector,
    dense_gate,
    dense_up,
    dense_down,
    exp_gate,
    exp_up,
    exp_down,
    routes,
    route_w,
):
    R, H = tokens.shape
    heads, hs = state.shape[1], state.shape[2]
    HW = heads * hs
    FE = exp_gate.shape[2]
    FD = dense_gate.shape[1]
    Z, C = EXPERTS, len(TRIPS)
    vm = pl.BlockSpec(memory_space=pltpu.VMEM)
    hbm = pl.BlockSpec(memory_space=pltpu.HBM)
    V = pltpu.VMEM
    sem = lambda *shape: pltpu.SemaphoreType.DMA(shape)
    operands = (
        tokens,
        norm_mix.reshape(1, -1),
        routes.T,
        route_w.T,
        norm_ffn.reshape(1, -1),
        gate_vector.reshape(-1, 128),
        state,
        w_query,
        w_key,
        w_value,
        w_out,
        dense_gate.T,
        dense_up.T,
        dense_down,
        exp_gate[0].T,
        exp_up[0].T,
        exp_down,
    )
    held = [pltpu.with_memory_space_constraint(x, pltpu.HBM) for x in operands]
    mixed, new_state = pl.pallas_call(
        kernel,
        out_shape=(pltpu.VMEM((R, H), BF16), pltpu.VMEM(state.shape, F32)),
        in_specs=[hbm] * 17,
        out_specs=(vm, vm),
        scratch_shapes=[
            V((R, H), BF16),
            V((1, 2 * H), F32),
            V((routes.shape[1], R), jnp.int32),
            V((routes.shape[1], R), BF16),
            V((1, H), F32),
            V((H // 128, 128), BF16),
            V((R, H), BF16),
            V((2, H, HW), BF16),
            V((2, H, HW), BF16),
            V((2, H, HW), BF16),
            V((2, HW, H), BF16),
            V((2, HW, H), BF16),
            V((2, FE, H), BF16),
            V((2, FE, H), BF16),
            V((2, FE, H), BF16),
            V(state.shape, F32),
            V((R, HW), BF16),
            V((R, HW), BF16),
            V((EXPERTS * SLOT, 128), F32),
            V((R, 128), F32),
            V((R, 128), F32),
            V((R, 128), F32),
            V((PLANE, 3, FD, H), BF16),
            V((PLANE, 32, H), BF16),
            V((PLANE, 32, H), BF16),
            V((PLANE, 32, H), BF16),
            V((2, 2, 128, H), BF16),
            V((2, 128, H), BF16),
            V((EXPERTS, SLOT, H), BF16),
            V((Z, SLOT, H), BF16),
            V((Z, R, H), BF16),
            V((C, PLANE, R, H), BF16),
            V((C, PLANE * R, 512), F32),
            V((C, PLANE * R, 512), BF16),
            V((C, PLANE * R, 512), BF16),
            V((2, Z * R, PLANE * 32), F32),
            V((2, Z * R, PLANE * 32), BF16),
            V((2, Z * R, PLANE * 32), BF16),
            V((C, PLANE, R, H), F32),
            V((C, PLANE, R, H), BF16),
            V((C, 2, 2, R, H), BF16),
            V((C, 2, 2, R, H), BF16),
            V((C, 2, 2, R, H), BF16),
            V((C, 2, 2, R, H), BF16),
            V((C, 2, R, H), F32),
            V((C, 2, R, H), BF16),
            V((C, R, H), BF16),
            V((C, R, H), BF16),
            V((C, R, H), BF16),
            V((C, R, H), BF16),
            V((Z, SLOT, H), BF16),
            V((EXPERTS, SLOT, H), BF16),
            V((R, H), F32),
            V((Z, R, H), BF16),
            V((Z, R, H), BF16),
            sem(32),
            sem(160),
            sem(160),
        ],
        compiler_params=pltpu.CompilerParams(
            collective_id=0, has_side_effects=True, vmem_limit_bytes=50 * 1024 * 1024
        ),
        name="layer",
    )(
        *held
    )
    return pl.pallas_call(
        store,
        out_shape=(
            jax.ShapeDtypeStruct((R, H), BF16),
            jax.ShapeDtypeStruct(state.shape, F32),
        ),
        in_specs=[vm, vm],
        out_specs=(hbm, hbm),
        scratch_shapes=[sem(2)],
        name="store",
    )(
        pltpu.with_memory_space_constraint(mixed, pltpu.VMEM),
        pltpu.with_memory_space_constraint(new_state, pltpu.VMEM),
    )


def solution(mesh):
    return jax.shard_map(
        body,
        mesh=mesh,
        in_specs=(
            P("ep", "tp"),
            P("ep", "tp", None, None),
            P(),
            P(None, "tp"),
            P(None, "tp"),
            P(None, "tp"),
            P("tp", None),
            P("tp"),
            P("tp"),
            P("tp", "ep"),
            P("tp", "ep"),
            P("ep", "tp"),
            P("ep", None, "tp"),
            P("ep", None, "tp"),
            P("ep", "tp", None),
            P("ep", None),
            P("ep", None),
        ),
        out_specs=(P("ep", "tp"), P("ep", "tp", None, None)),
        check_vma=False,
    )
```

```python
import functools

import jax
import jax.numpy as jnp
from jax import lax
from jax.experimental import pallas as pl
from jax.experimental.pallas import tpu as pltpu
from jax.sharding import PartitionSpec as P

EXPERTS = 8
CAP = 5
SLOT = 8
SIDE = 4
PLANE = SIDE * SIDE
TRIPS = ((0, 1, 7), (3, 5, 4), (2, 6))
epsilon = 1e-06
MESH = pl.DeviceIdType.MESH
F32 = jnp.float32
BF16 = jnp.bfloat16


def dot(a, b):
    return jnp.dot(a, b, preferred_element_type=F32)


def dot_t(a, b):
    return lax.dot_general(a, b, (((1,), (1,)), ((), ())), preferred_element_type=F32)


def silu(v):
    return v / (1.0 + jnp.exp(-v))


def iota(shape, dim):
    return lax.broadcasted_iota(jnp.int32, shape, dim)


def kernel(
    tokens_h,
    norm_mix_h,
    routes_h,
    route_w_h,
    norm_ffn_h,
    gate_vec_h,
    state,
    w_query,
    w_key,
    w_value,
    w_out,
    dense_gate,
    dense_up,
    dense_down,
    exp_gate,
    exp_up,
    exp_down,
    mixed,
    ns,
    tokens,
    norm_mix,
    routes,
    route_w,
    norm_ffn,
    gate_vec,
    tok_p,
    wq,
    wk,
    wv,
    wo_o,
    wo_p,
    eg,
    eu,
    ed,
    st,
    ho_o,
    ho_p,
    sel_m,
    comb_m,
    lg_s,
    lg_r,
    wbuf,
    wdg,
    wdu,
    wdd,
    w1,
    w2,
    xs,
    zr,
    xz,
    xe,
    pe_o,
    pe_s,
    pe_r,
    pd_o,
    pd_s,
    pd_r,
    y32,
    yb,
    rb,
    rd,
    rs,
    rf,
    sa,
    sb,
    ab,
    ad,
    ax,
    af,
    zs,
    zret,
    yz0,
    yzs,
    yzr,
    lsem,
    ssem,
    rsem,
):
    R, H = tokens.shape
    D = 2 * H
    heads, hs = state.shape[1], state.shape[2]
    HW = heads * hs
    FE = eg.shape[1]
    FD = wbuf.shape[2]
    Z = EXPERTS
    me = lax.axis_index("ep")
    tp = lax.axis_index("tp")
    other = 1 - tp
    z, y_at, x_at = me // PLANE, (me // SIDE) % SIDE, me % SIDE

    def in_plane(dy, dx):
        return {
            "ep": z * PLANE + ((y_at + dy + SIDE) % SIDE) * SIDE + (x_at + dx + SIDE) % SIDE,
            "tp": tp,
        }

    first = {d: in_plane(tp * d, other * d) for d in (1, -1)}
    second = {d: in_plane(other * d, tp * d) for d in (1, -1)}
    zpeer = [{"ep": ((z + i) % Z) * PLANE + me % PLANE, "tp": tp} for i in range(Z)]
    partner = {"ep": me, "tp": other}

    def place(p):
        turned = (p % SIDE) * SIDE + p // SIDE
        return p + tp * (turned - p)

    own = pl.ds(pl.multiple_of(tp * H, H), H)
    oth = pl.ds(pl.multiple_of(other * H, H), H)

    sent = []

    def remote(src, dst, dev):
        k = len(sent)
        copy = pltpu.make_async_remote_copy(
            src_ref=src,
            dst_ref=dst,
            send_sem=ssem.at[k],
            recv_sem=rsem.at[k],
            device_id=dev,
            device_id_type=MESH,
        )
        copy.start()
        sent.append(copy)
        return copy

    local = {}

    def load(name, src, dst):
        copy = pltpu.make_async_copy(src, dst, lsem.at[len(local)])
        copy.start()
        local[name] = copy

    class Gather:
        def __init__(self, buf, via):
            self.buf, self.via = buf, via
            self.up, self.down = {}, {}

        def spread(self, a):
            at = self.buf.at
            self.up[a] = remote(at[a], at[3 * SIDE + a], second[1])
            self.down[a] = remote(at[a], at[SIDE + a], second[-1])

        def start(self):
            at = self.buf.at
            self.f_up = remote(at[0], at[3], first[1])
            self.f_down = remote(at[0], at[1], first[-1])
            self.spread(0)

        def one(self):
            at = self.buf.at
            self.f_up.wait_recv()
            if self.via > 0:
                self.f_two = remote(at[3], at[2], first[1])
            self.spread(3)
            self.f_down.wait_recv()
            if self.via < 0:
                self.f_two = remote(at[1], at[2], first[-1])
            self.spread(1)

        def two(self):
            self.f_two.wait_recv()
            self.spread(2)

        def relay(self, todo):
            at = self.buf.at
            for a in todo:
                self.up[a].wait_recv()
                if a in (0, 1):
                    self.up[a + SIDE] = remote(at[3 * SIDE + a], at[2 * SIDE + a], second[1])
                self.down[a].wait_recv()
                if a in (2, 3):
                    self.up[a + SIDE] = remote(at[SIDE + a], at[2 * SIDE + a], second[-1])

        def finish(self):
            for a in range(SIDE):
                self.up[a + SIDE].wait_recv()

    small = (
        (tokens_h, tokens),
        (norm_mix_h, norm_mix),
        (routes_h, routes),
        (route_w_h, route_w),
        (norm_ffn_h, norm_ffn),
        (gate_vec_h, gate_vec),
    )
    barrier = pltpu.get_barrier_semaphore()
    greeted = [partner, first[1], first[-1], second[1], second[-1]] + zpeer[1:]
    for dev in greeted:
        pl.semaphore_signal(barrier, inc=1, device_id=dev, device_id_type=MESH)

    for t, (src, dst) in enumerate(small):
        load(f"s{t}", src, dst)
    for t, src in enumerate((dense_gate, dense_up, dense_down)):
        load(f"d{t}", src, wbuf.at[0, t])
    for t, (src, dst) in enumerate(((w_query, wq), (w_key, wk), (w_value, wv))):
        load(f"p{t}o", src.at[own, :], dst.at[0])
        load(f"p{t}p", src.at[oth, :], dst.at[1])
    load("st", state, st)
    load("wo0", w_out.at[:, own], wo_o.at[0])
    load("wo1", w_out.at[:, oth], wo_o.at[1])
    load("eg", exp_gate.at[:, own], eg.at[tp])
    load("eu", exp_up.at[:, own], eu.at[tp])
    load("ed", exp_down.at[0, :, own], ed.at[tp])

    local["s0"].wait()
    pl.semaphore_wait(barrier, len(greeted))

    c_tok = remote(tokens, tok_p, partner)
    weights = Gather(wbuf, 1)
    for t in range(3):
        local[f"d{t}"].wait()
    weights.start()
    c_wo0 = remote(w_out.at[:, oth], wo_p.at[0], partner)
    c_wo1 = remote(w_out.at[:, own], wo_p.at[1], partner)
    c_eg = remote(exp_gate.at[:, oth], eg.at[tp], partner)
    c_eu = remote(exp_up.at[:, oth], eu.at[tp], partner)
    c_ed = remote(exp_down.at[0, :, oth], ed.at[tp], partner)

    for t in (2, 3):
        local[f"s{t}"].wait()
    row_id = iota((EXPERTS, R), 0)
    wt = jnp.zeros((EXPERTS, R), F32)
    member = jnp.zeros((EXPERTS, R), F32)
    named = routes[...]
    gains = route_w[...].astype(F32)
    for t in range(routes.shape[0]):
        hit = row_id == named[t : t + 1, :]
        wt = wt + jnp.where(hit, gains[t : t + 1, :], 0.0)
        member = member + jnp.where(hit, 1.0, 0.0)
    blank = jnp.zeros((EXPERTS, 128 - R), F32)
    wt = jnp.concatenate([wt, blank], axis=1)
    member = jnp.concatenate([member, blank], axis=1)
    before = jnp.where(iota((128, 128), 0) < iota((128, 128), 1), 1.0, 0.0).astype(BF16)
    rank = dot(member.astype(BF16), before)
    slot_id = iota((SLOT, 128), 0).astype(F32)
    picks, scaled = [], []
    for e in range(EXPERTS):
        pick = jnp.where(rank[e : e + 1] == slot_id, member[e : e + 1], 0.0)
        picks.append(pick)
        scaled.append(pick * wt[e : e + 1])
    sel_m[...] = jnp.concatenate(picks, axis=0)
    scaled.append(jnp.zeros((128 - EXPERTS * SLOT, 128), F32))
    comb_m[...] = jnp.concatenate(scaled, axis=0).T[:R]
    for t in (1, 4, 5):
        local[f"s{t}"].wait()

    tok_f = tokens[...].astype(F32)
    c_tok.wait_recv()
    tok_pf = tok_p[...].astype(F32)
    total = jnp.sum(tok_f * tok_f, axis=1, keepdims=True) + jnp.sum(
        tok_pf * tok_pf, axis=1, keepdims=True
    )
    scale = lax.rsqrt(total / D + epsilon)
    gain_o = norm_mix[:, own]
    gain_p = norm_mix[:, oth]
    nx_o = (tok_f * scale * gain_o).astype(BF16)
    nx_p = (tok_pf * scale * gain_p).astype(BF16)
    proj = []
    for t, w in enumerate((wq, wk, wv)):
        local[f"p{t}o"].wait()
        part = dot(nx_o, w[0])
        local[f"p{t}p"].wait()
        proj.append((part + dot(nx_p, w[1])).astype(BF16).astype(F32))
    q, k, v = proj
    k = k * hs ** (-0.5)
    pad = jnp.zeros((128 - R, HW), F32)
    q_t = jnp.concatenate([q, pad], axis=0).T
    k_t = jnp.concatenate([k, pad], axis=0).T
    head_id = tp * heads
    local["st"].wait()
    decays = []
    for h in range(heads):
        cols = slice(h * hs, (h + 1) * hs)
        idv = jnp.zeros((1, 128), F32) + (head_id + h).astype(F32)
        decay = 1.0 - jnp.exp2(-3.0 - 2.0 * idv)
        decays.append(decay)
        rows = []
        for s in range(R):
            rows.append(jnp.sum(st[s, h] * q_t[cols, s : s + 1], axis=0, keepdims=True))
        qs = jnp.concatenate(rows, axis=0)
        qk = jnp.sum(q[:, cols] * k[:, cols], axis=1, keepdims=True)
        read = decay * qs + qk * v[:, cols]
        centre = jnp.mean(read, axis=1, keepdims=True)
        dev = read - centre
        spread = jnp.mean(dev * dev, axis=1, keepdims=True)
        ho_o[:, cols] = (dev * lax.rsqrt(spread + epsilon)).astype(BF16)
    c_ho = remote(ho_o, ho_p, partner)
    ho = ho_o[...]
    local["wo0"].wait()
    local["wo1"].wait()
    a_o = dot(ho, wo_o[0]).astype(BF16).astype(F32)
    a_p = dot(ho, wo_o[1]).astype(BF16).astype(F32)
    weights.one()
    c_wo0.wait_recv()
    c_wo1.wait_recv()
    c_ho.wait_recv()
    hp = ho_p[...]
    a_o = a_o + dot(hp, wo_p[0]).astype(BF16).astype(F32)
    a_p = a_p + dot(hp, wo_p[1]).astype(BF16).astype(F32)
    after = (tok_f + a_o).astype(BF16).astype(F32)
    after_p = (tok_pf + a_p).astype(BF16).astype(F32)
    squares = jnp.sum(after * after, axis=1, keepdims=True) + jnp.sum(
        after_p * after_p, axis=1, keepdims=True
    )
    normed = (after * lax.rsqrt(squares / D + epsilon) * norm_ffn[...]).astype(BF16)

    chosen = dot(sel_m[:, :R].astype(BF16), normed).astype(BF16)
    xs[...] = chosen.astype(F32).reshape(EXPERTS, SLOT, H).astype(BF16)
    xz[0] = normed
    c_zr = {}
    for i in (1, 7, 4, 3, 5, 2, 6):
        c_zr[i] = remote(xs.at[(z + i) % Z], zr.at[Z - i], zpeer[i])
    c_xz = {}
    for i in (1, 7, 2, 6, 3, 5, 4):
        c_xz[i] = remote(xz.at[0], xz.at[Z - i], zpeer[i])
    gate_row = gate_vec[...].astype(F32)
    gate_row = jnp.concatenate([gate_row[r : r + 1] for r in range(H // 128)], axis=1)
    logit = jnp.sum(normed.astype(F32) * gate_row, axis=1, keepdims=True)
    lg_s[...] = logit + jnp.zeros((R, 128), F32)
    c_lg = remote(lg_s, lg_r, partner)
    weights.relay((0,))

    def new_state(h):
        cols = slice(h * hs, (h + 1) * hs)
        for s in range(R):
            ns[s, h] = decays[h] * st[s, h] + k_t[cols, s : s + 1] * v[s : s + 1, cols]

    new_state(0)

    for name in ("eg", "eu", "ed"):
        local[name].wait()
    for copy in (c_eg, c_eu, c_ed):
        copy.wait_recv()
    for t in range(2):
        for src, dst in ((eg, w1.at[0, t]), (eu, w1.at[1, t]), (ed, w2.at[t])):
            dst[:FE] = src[t]
            dst[FE:] = jnp.zeros((128 - FE, H), BF16)
    new_state(1)

    chunks = [Gather(xe.at[c], 1 if c % 2 == 0 else -1) for c in range(len(TRIPS))]

    def pack(c):
        parts = []
        for i in TRIPS[c]:
            if i == 0:
                parts.append(xs[z].astype(F32))
            else:
                c_zr[Z - i].wait_recv()
                parts.append(zr[i].astype(F32))
        parts.append(jnp.zeros((32 - SLOT * len(parts), H), F32))
        rows = jnp.concatenate(parts, axis=0).astype(BF16)
        r, s = iota((R, 32), 0), iota((R, 32), 1)
        take = jnp.zeros((R, 32), F32)
        for j in range(len(TRIPS[c])):
            hit = (s - SLOT * j == r - CAP * j) & (r >= CAP * j) & (r < CAP * (j + 1))
            take = take + jnp.where(hit, 1.0, 0.0)
        xe[c, 0] = dot(take.astype(BF16), rows).astype(BF16)
        chunks[c].start()

    pack(0)
    weights.two()
    pack(2)
    pack(1)
    weights.relay((3, 1))
    chunks[0].one()
    chunks[0].relay((0,))
    chunks[2].one()
    weights.relay((2,))
    chunks[0].two()
    chunks[2].relay((0,))
    chunks[1].one()
    chunks[0].relay((3, 1))
    chunks[1].relay((0,))
    chunks[2].two()
    chunks[2].relay((3, 1))
    chunks[0].relay((2,))
    chunks[1].two()

    c_pe = {}

    def before_act(c):
        chunks[c].finish()
        pre = dot_t(xe[c].reshape(PLANE * R, H), w1[...].reshape(4 * 128, H))
        pe_o[c] = pre
        for b in range(SIDE):
            for a in range(SIDE):
                f = SIDE * b + a
                pe_s[c, SIDE * a + b] = pre[f * R : (f + 1) * R].astype(BF16)
        c_pe[c] = remote(pe_s.at[c], pe_r.at[c], partner)

    def act(c):
        c_pe[c].wait_recv()
        pre = pe_o[c] + pe_r[c].reshape(PLANE * R, 512).astype(F32)
        hidden = (silu(pre[:, :256]) * pre[:, 256:]).astype(BF16)
        down = w2[...].reshape(256, H)
        yb[c] = dot(hidden[6 * R : 14 * R], down).astype(BF16).reshape(8, R, H)
        at = yb.at
        c_rb[c] = (
            remote(at[c, pl.ds(2, 2)], rb.at[c, 0], second[1]),
            remote(at[c, pl.ds(4, 2)], rb.at[c, 1], second[-1]),
        )
        c_rd[c] = (
            remote(at[c, pl.ds(0, 2)], rd.at[c, 0], second[1]),
            remote(at[c, pl.ds(6, 2)], rd.at[c, 1], second[-1]),
        )
        y32[c, 4:6] = dot(hidden[4 * R : 6 * R], down).reshape(2, R, H)
        y32[c, 6:8] = dot(hidden[14 * R :], down).reshape(2, R, H)
        y32[c, 0:4] = dot(hidden[: 4 * R], down).reshape(4, R, H)

    c_rb, c_rd, c_rf, c_ab, c_ad, c_af = {}, {}, {}, {}, {}, {}

    def sum_relay(c):
        c_rb[c][0].wait_recv()
        rs[c, 0] = (y32[c, 4:6] + rb[c, 0].astype(F32)).astype(BF16)
        up = remote(rs.at[c, 0], rf.at[c, 0], second[1])
        c_rb[c][1].wait_recv()
        rs[c, 1] = (y32[c, 6:8] + rb[c, 1].astype(F32)).astype(BF16)
        c_rf[c] = (up, remote(rs.at[c, 1], rf.at[c, 1], second[-1]))

    def sum_second(c):
        via = chunks[c].via
        near, far = (1, 3) if via > 0 else (3, 1)
        c_rd[c][1].wait_recv()
        c_rf[c][0].wait_recv()
        low = y32[c, 0:2] + rf[c, 0].astype(F32) + rd[c, 1].astype(F32)
        c_rd[c][0].wait_recv()
        c_rf[c][1].wait_recv()
        high = y32[c, 2:4] + rf[c, 1].astype(F32) + rd[c, 0].astype(F32)
        total = (low[0], low[1], high[0], high[1])
        sb[c, 0] = total[2].astype(BF16)
        c_ab[c] = remote(sb.at[c, 0], ab.at[c], first[via])
        sb[c, 1] = total[far].astype(BF16)
        c_ad[c] = remote(sb.at[c, 1], ad.at[c], first[-via])
        sa[c, 0] = total[0]
        sa[c, 1] = total[near]

    def sum_two(c):
        c_ab[c].wait_recv()
        ax[c] = (sa[c, 1] + ab[c].astype(F32)).astype(BF16)
        c_af[c] = remote(ax.at[c], af.at[c], first[chunks[c].via])

    c_ret = {}

    def give_back(c):
        c_ad[c].wait_recv()
        c_af[c].wait_recv()
        total = (sa[c, 0] + ad[c].astype(F32) + af[c].astype(F32)).astype(BF16)
        n = len(TRIPS[c])
        s, r = iota((32, R), 0), iota((32, R), 1)
        put = jnp.zeros((32, R), F32)
        for j in range(n):
            hit = (s - SLOT * j == r - CAP * j) & (r >= CAP * j) & (r < CAP * (j + 1))
            put = put + jnp.where(hit, 1.0, 0.0)
        rows = dot(put.astype(BF16), total)
        for j, i in enumerate(TRIPS[c]):
            block = rows[j * SLOT : (j + 1) * SLOT].astype(BF16)
            if i == 0:
                zret[z] = block
            else:
                zs[i] = block
                c_ret[i] = remote(zs.at[i], zret.at[z], zpeer[i])

    weights.finish()

    for p in range(PLANE):
        for t, dst in enumerate((wdg, wdu, wdd)):
            dst[p, :FD] = wbuf[place(p), t]
            dst[p, FD:] = jnp.zeros((32 - FD, H), BF16)

    def dense_before():
        for i in range(1, Z):
            c_xz[i].wait_recv()
        x = xz[...].reshape(Z * R, H)
        for t, w in enumerate((wdg, wdu)):
            pre = dot_t(x, w[...].reshape(PLANE * 32, H))
            pd_o[t] = pre
            pd_s[t] = pre.astype(BF16)
        return remote(pd_s, pd_r, partner)

    def dense_act():
        gate = pd_o[0] + pd_r[0].astype(F32)
        up = pd_o[1] + pd_r[1].astype(F32)
        y = dot((silu(gate) * up).astype(BF16), wdd[...].reshape(PLANE * 32, H))
        yz0[...] = y[:R]
        yzs[...] = y.astype(BF16).reshape(Z, R, H)
        return {i: remote(yzs.at[i], yzr.at[Z - i], zpeer[i]) for i in (4, 3, 5, 2, 6, 1, 7)}

    chunks[1].relay((3, 1))
    chunks[2].relay((2,))
    before_act(0)
    c_pd = dense_before()
    chunks[1].relay((2,))
    before_act(2)
    act(0)
    before_act(1)
    c_pd.wait_recv()
    c_yz = dense_act()
    act(1)
    sum_relay(0)
    act(2)
    sum_relay(1)
    sum_second(0)
    sum_relay(2)
    sum_second(1)
    sum_two(0)
    sum_second(2)
    sum_two(1)
    give_back(0)
    sum_two(2)
    give_back(1)
    give_back(2)

    c_lg.wait_recv()
    open_ = 1.0 / (1.0 + jnp.exp(-(lg_s[:, :1] + lg_r[:, :1])))
    dense = yz0[...]
    for i in range(1, Z):
        c_yz[i].wait_recv()
        dense = dense + yzr[Z - i].astype(F32)
    for i in range(1, Z):
        c_ret[i].wait_recv()
    back = zret[...].astype(F32).reshape(EXPERTS * SLOT, H).astype(BF16)
    moe = dot(comb_m[:, : EXPERTS * SLOT].astype(BF16), back)
    mixed[...] = (after + moe + open_ * dense).astype(BF16)
    for copy in sent:
        copy.wait_send()


def store(a_in, b_in, a_out, b_out, sems):
    first = pltpu.make_async_copy(b_in, b_out, sems.at[0])
    second = pltpu.make_async_copy(a_in, a_out, sems.at[1])
    first.start()
    second.start()
    first.wait()
    second.wait()


def body(
    tokens,
    state,
    norm_mix,
    w_query,
    w_key,
    w_value,
    w_out,
    norm_ffn,
    gate_vector,
    dense_gate,
    dense_up,
    dense_down,
    exp_gate,
    exp_up,
    exp_down,
    routes,
    route_w,
):
    R, H = tokens.shape
    heads, hs = state.shape[1], state.shape[2]
    HW = heads * hs
    FE = exp_gate.shape[2]
    FD = dense_gate.shape[1]
    Z, C = EXPERTS, len(TRIPS)
    vm = pl.BlockSpec(memory_space=pltpu.VMEM)
    hbm = pl.BlockSpec(memory_space=pltpu.HBM)
    V = pltpu.VMEM
    sem = lambda *shape: pltpu.SemaphoreType.DMA(shape)
    operands = (
        tokens,
        norm_mix.reshape(1, -1),
        routes.T,
        route_w.T,
        norm_ffn.reshape(1, -1),
        gate_vector.reshape(-1, 128),
        state,
        w_query,
        w_key,
        w_value,
        w_out,
        dense_gate.T,
        dense_up.T,
        dense_down,
        exp_gate[0].T,
        exp_up[0].T,
        exp_down,
    )
    held = [pltpu.with_memory_space_constraint(x, pltpu.HBM) for x in operands]
    mixed, new_state = pl.pallas_call(
        kernel,
        out_shape=(pltpu.VMEM((R, H), BF16), pltpu.VMEM(state.shape, F32)),
        in_specs=[hbm] * 17,
        out_specs=(vm, vm),
        scratch_shapes=[
            V((R, H), BF16),
            V((1, 2 * H), F32),
            V((routes.shape[1], R), jnp.int32),
            V((routes.shape[1], R), BF16),
            V((1, H), F32),
            V((H // 128, 128), BF16),
            V((R, H), BF16),
            V((2, H, HW), BF16),
            V((2, H, HW), BF16),
            V((2, H, HW), BF16),
            V((2, HW, H), BF16),
            V((2, HW, H), BF16),
            V((2, FE, H), BF16),
            V((2, FE, H), BF16),
            V((2, FE, H), BF16),
            V(state.shape, F32),
            V((R, HW), BF16),
            V((R, HW), BF16),
            V((EXPERTS * SLOT, 128), F32),
            V((R, 128), F32),
            V((R, 128), F32),
            V((R, 128), F32),
            V((PLANE, 3, FD, H), BF16),
            V((PLANE, 32, H), BF16),
            V((PLANE, 32, H), BF16),
            V((PLANE, 32, H), BF16),
            V((2, 2, 128, H), BF16),
            V((2, 128, H), BF16),
            V((EXPERTS, SLOT, H), BF16),
            V((Z, SLOT, H), BF16),
            V((Z, R, H), BF16),
            V((C, PLANE, R, H), BF16),
            V((C, PLANE * R, 512), F32),
            V((C, PLANE, R, 512), BF16),
            V((C, PLANE, R, 512), BF16),
            V((2, Z * R, PLANE * 32), F32),
            V((2, Z * R, PLANE * 32), BF16),
            V((2, Z * R, PLANE * 32), BF16),
            V((C, 8, R, H), F32),
            V((C, 8, R, H), BF16),
            V((C, 2, 2, R, H), BF16),
            V((C, 2, 2, R, H), BF16),
            V((C, 2, 2, R, H), BF16),
            V((C, 2, 2, R, H), BF16),
            V((C, 2, R, H), F32),
            V((C, 2, R, H), BF16),
            V((C, R, H), BF16),
            V((C, R, H), BF16),
            V((C, R, H), BF16),
            V((C, R, H), BF16),
            V((Z, SLOT, H), BF16),
            V((EXPERTS, SLOT, H), BF16),
            V((R, H), F32),
            V((Z, R, H), BF16),
            V((Z, R, H), BF16),
            sem(32),
            sem(160),
            sem(160),
        ],
        compiler_params=pltpu.CompilerParams(
            collective_id=0, has_side_effects=True, vmem_limit_bytes=50 * 1024 * 1024
        ),
        name="layer",
    )(
        *held
    )
    return pl.pallas_call(
        store,
        out_shape=(
            jax.ShapeDtypeStruct((R, H), BF16),
            jax.ShapeDtypeStruct(state.shape, F32),
        ),
        in_specs=[vm, vm],
        out_specs=(hbm, hbm),
        scratch_shapes=[sem(2)],
        name="store",
    )(
        pltpu.with_memory_space_constraint(mixed, pltpu.VMEM),
        pltpu.with_memory_space_constraint(new_state, pltpu.VMEM),
    )


def solution(mesh):
    return jax.shard_map(
        body,
        mesh=mesh,
        in_specs=(
            P("ep", "tp"),
            P("ep", "tp", None, None),
            P(),
            P(None, "tp"),
            P(None, "tp"),
            P(None, "tp"),
            P("tp", None),
            P("tp"),
            P("tp"),
            P("tp", "ep"),
            P("tp", "ep"),
            P("ep", "tp"),
            P("ep", None, "tp"),
            P("ep", None, "tp"),
            P("ep", "tp", None),
            P("ep", None),
            P("ep", None),
        ),
        out_specs=(P("ep", "tp"), P("ep", "tp", None, None)),
        check_vma=False,
    )
```

```python
import functools

import jax
import jax.numpy as jnp
from jax import lax
from jax.experimental import pallas as pl
from jax.experimental.pallas import tpu as pltpu
from jax.sharding import PartitionSpec as P

EXPERTS = 8
CAP = 5
SLOT = 8
SIDE = 4
PLANE = SIDE * SIDE
NEAR = (0, 1, 7, 2, 6, 3, 5, 4)
PACKED = (4, 3, 5, 2, 6, 1, 7, 0)
CHUNKS = (24, 16, 16)
GROUPS = 32
LOADS = 21
epsilon = 1e-06
MESH = pl.DeviceIdType.MESH
F32 = jnp.float32
BF16 = jnp.bfloat16


def dot(a, b):
    return jnp.dot(a, b, preferred_element_type=F32)


def dot_t(a, b):
    return lax.dot_general(a, b, (((1,), (1,)), ((), ())), preferred_element_type=F32)


def silu(v):
    return v / (1.0 + jnp.exp(-v))


def iota(shape, dim):
    return lax.broadcasted_iota(jnp.int32, shape, dim)


def kernel(
    tokens_h,
    norm_mix_h,
    routes_h,
    route_w_h,
    norm_ffn_h,
    gate_vec_h,
    state,
    w_query,
    w_key,
    w_value,
    w_out,
    dense_gate,
    dense_up,
    dense_down,
    exp_gate,
    exp_up,
    exp_down,
    mixed,
    ns,
    tokens,
    norm_mix,
    routes,
    route_w,
    norm_ffn,
    gate_vec,
    tok_p,
    wq,
    wk,
    wv,
    wo_o,
    wo_p,
    eg,
    eu,
    ed,
    st,
    ho_o,
    ho_p,
    sel_m,
    scl_m,
    lg_s,
    lg_r,
    wbuf,
    w1,
    w2,
    w1d,
    w2d,
    xs,
    zr,
    xe_a,
    xe_b,
    xe_d,
    pe_o_a,
    pe_o_b,
    pe_o_d,
    pe_s_a,
    pe_s_b,
    pe_s_d,
    pe_r_a,
    pe_r_b,
    pe_r_d,
    y_a,
    y_b,
    y_d,
    yb_a,
    yb_b,
    yb_d,
    rb_a,
    rb_b,
    rb_d,
    sb_a,
    sb_b,
    sb_d,
    ra_a,
    ra_b,
    ra_d,
    tot,
    zs,
    zret,
    lsem,
    ssem,
    rsem,
):
    R, H = tokens.shape
    D = 2 * H
    heads, hs = state.shape[1], state.shape[2]
    HW = heads * hs
    FE = eg.shape[1]
    FD = wbuf.shape[2]
    Z = EXPERTS
    me = lax.axis_index("ep")
    tp = lax.axis_index("tp")
    other = 1 - tp
    z, y_at, x_at = me // PLANE, (me // SIDE) % SIDE, me % SIDE

    def in_plane(dy, dx):
        return {
            "ep": z * PLANE + ((y_at + dy + SIDE) % SIDE) * SIDE + (x_at + dx + SIDE) % SIDE,
            "tp": tp,
        }

    first = {d: in_plane(tp * d, other * d) for d in (1, -1, 2)}
    second = {d: in_plane(other * d, tp * d) for d in (1, -1, 2)}
    zpeer = [{"ep": ((z + i) % Z) * PLANE + me % PLANE, "tp": tp} for i in range(Z)]
    partner = {"ep": me, "tp": other}

    own = pl.ds(pl.multiple_of(tp * H, H), H)
    oth = pl.ds(pl.multiple_of(other * H, H), H)

    sent = []

    class Group:
        def __init__(self, whole):
            self.k, self.whole = len(sent), whole
            sent.append(self)

        def copy(self, src, dst, dev):
            self.dev = dev
            return pltpu.make_async_remote_copy(
                src_ref=src,
                dst_ref=dst,
                send_sem=ssem.at[self.k],
                recv_sem=rsem.at[self.k],
                device_id=dev,
                device_id_type=MESH,
            )

        def add(self, src, dst, dev):
            self.copy(src, dst, dev).start()

        def wait_recv(self):
            self.copy(self.whole, self.whole, self.dev).wait_recv()

        def wait_send(self):
            self.copy(self.whole, self.whole, self.dev).wait_send()

    def remote(src, dst, dev):
        group = Group(dst)
        group.add(src, dst, dev)
        return group

    local = {}

    def load(name, src, dst):
        copy = pltpu.make_async_copy(src, dst, lsem.at[len(local)])
        copy.start()
        local[name] = copy

    HOPS = ((1, 1), (-1, 2), (2, 3))
    BACK = ((2, 3), (-1, 1), (1, 2))

    class Gather:
        def __init__(self, buf):
            self.at = buf.at

        def spread(self, *todo):
            for d, b in HOPS:
                for a in todo:
                    self.across.add(self.at[a], self.at[SIDE * b + a], second[d])

        def start(self):
            at = self.at
            self.near, self.far = Group(at[pl.ds(1, 2)]), Group(at[3])
            self.across = Group(at[pl.ds(SIDE, 3 * SIDE)])
            self.near.add(at[0], at[1], first[1])
            self.near.add(at[0], at[2], first[-1])
            self.far.add(at[0], at[3], first[2])
            self.spread(0)

        def go(self):
            self.near.wait_recv()
            self.spread(1, 2)
            self.far.wait_recv()
            self.spread(3)

    class Ring:
        def __init__(self, buf):
            self.at, self.step = buf.at, 0

        def start(self):
            at, t = self.at, self.step
            if t:
                self.group.wait_recv()
            up, down = max(0, 2 * t), max(0, 2 * t - 1)
            if t < 3:
                self.group = Group(at[pl.ds(2 * t + 1, 2)])
                self.group.add(at[up], at[2 * t + 2], zpeer[1])
                self.group.add(at[down], at[2 * t + 1], zpeer[-1])
            elif t == 3:
                self.group = Group(at[7])
                self.group.add(at[up, pl.ds(0, 2)], at[7, pl.ds(0, 2)], zpeer[1])
                self.group.add(at[down, pl.ds(2, 1)], at[7, pl.ds(2, 1)], zpeer[-1])
            self.step = t + 1

    small = (
        (tokens_h, tokens),
        (norm_mix_h, norm_mix),
        (routes_h, routes),
        (route_w_h, route_w),
        (norm_ffn_h, norm_ffn),
        (gate_vec_h, gate_vec),
    )
    barrier = pltpu.get_barrier_semaphore()
    greeted = [partner, *first.values(), *second.values()] + zpeer[1:]
    for dev in greeted:
        pl.semaphore_signal(barrier, inc=1, device_id=dev, device_id_type=MESH)

    for t, (src, dst) in enumerate(small):
        load(f"s{t}", src, dst)
    for t, src in enumerate((dense_gate, dense_up, dense_down)):
        load(f"d{t}", src, wbuf.at[0, t])
    for t, (src, dst) in enumerate(((w_query, wq), (w_key, wk), (w_value, wv))):
        load(f"p{t}o", src.at[own, :], dst.at[0])
        load(f"p{t}p", src.at[oth, :], dst.at[1])
    load("st", state, st)
    load("wo0", w_out.at[:, own], wo_o.at[0])
    load("wo1", w_out.at[:, oth], wo_o.at[1])
    load("eg", exp_gate.at[:, own], eg.at[tp])
    load("eu", exp_up.at[:, own], eu.at[tp])
    load("ed", exp_down.at[0, :, own], ed.at[tp])

    local["s0"].wait()
    pl.semaphore_wait(barrier, len(greeted))

    c_tok = remote(tokens, tok_p, partner)
    weights = Ring(wbuf)
    for t in range(3):
        local[f"d{t}"].wait()
    weights.start()
    c_wo = Group(wo_p)
    c_wo.add(w_out.at[:, oth], wo_p.at[0], partner)
    c_wo.add(w_out.at[:, own], wo_p.at[1], partner)
    c_eg = remote(exp_gate.at[:, oth], eg.at[tp], partner)
    c_eu = remote(exp_up.at[:, oth], eu.at[tp], partner)
    c_ed = remote(exp_down.at[0, :, oth], ed.at[tp], partner)

    for t in (2, 3):
        local[f"s{t}"].wait()
    row_id = iota((EXPERTS, R), 0)
    wt = jnp.zeros((EXPERTS, R), F32)
    member = jnp.zeros((EXPERTS, R), F32)
    named = routes[...]
    gains = route_w[...].astype(F32)
    for t in range(routes.shape[0]):
        hit = row_id == named[t : t + 1, :]
        wt = wt + jnp.where(hit, gains[t : t + 1, :], 0.0)
        member = member + jnp.where(hit, 1.0, 0.0)
    blank = jnp.zeros((EXPERTS, 128 - R), F32)
    wt = jnp.concatenate([wt, blank], axis=1)
    member = jnp.concatenate([member, blank], axis=1)
    before = jnp.where(iota((128, 128), 0) < iota((128, 128), 1), 1.0, 0.0).astype(BF16)
    rank = dot(member.astype(BF16), before)
    slot_id = iota((SLOT, 128), 0).astype(F32)
    picks = []
    for e in range(EXPERTS):
        pick = jnp.where(rank[e : e + 1] == slot_id, member[e : e + 1], 0.0)
        picks.append(pick)
        scl_m[e] = pick * wt[e : e + 1]
    sel_m[...] = jnp.concatenate(picks, axis=0)
    for t in (1, 4, 5):
        local[f"s{t}"].wait()

    tok_f = tokens[...].astype(F32)
    c_tok.wait_recv()
    tok_pf = tok_p[...].astype(F32)
    total = jnp.sum(tok_f * tok_f, axis=1, keepdims=True) + jnp.sum(
        tok_pf * tok_pf, axis=1, keepdims=True
    )
    scale = lax.rsqrt(total / D + epsilon)
    gain_o = norm_mix[:, own]
    gain_p = norm_mix[:, oth]
    nx_o = (tok_f * scale * gain_o).astype(BF16)
    nx_p = (tok_pf * scale * gain_p).astype(BF16)
    proj = []
    for t, w in enumerate((wq, wk, wv)):
        local[f"p{t}o"].wait()
        part = dot(nx_o, w[0])
        local[f"p{t}p"].wait()
        proj.append((part + dot(nx_p, w[1])).astype(BF16).astype(F32))
    q, k, v = proj
    k = k * hs ** (-0.5)
    pad = jnp.zeros((128 - R, HW), F32)
    q_t = jnp.concatenate([q, pad], axis=0).T
    k_t = jnp.concatenate([k, pad], axis=0).T
    head_id = tp * heads
    local["st"].wait()
    decays = []
    for h in range(heads):
        cols = slice(h * hs, (h + 1) * hs)
        idv = jnp.zeros((1, 128), F32) + (head_id + h).astype(F32)
        decay = 1.0 - jnp.exp2(-3.0 - 2.0 * idv)
        decays.append(decay)
        rows = []
        for s in range(R):
            rows.append(jnp.sum(st[s, h] * q_t[cols, s : s + 1], axis=0, keepdims=True))
        qs = jnp.concatenate(rows, axis=0)
        qk = jnp.sum(q[:, cols] * k[:, cols], axis=1, keepdims=True)
        read = decay * qs + qk * v[:, cols]
        centre = jnp.mean(read, axis=1, keepdims=True)
        dev = read - centre
        spread = jnp.mean(dev * dev, axis=1, keepdims=True)
        ho_o[:, cols] = (dev * lax.rsqrt(spread + epsilon)).astype(BF16)
    c_ho = remote(ho_o, ho_p, partner)
    ho = ho_o[...]
    local["wo0"].wait()
    local["wo1"].wait()
    a_o = dot(ho, wo_o[0]).astype(BF16).astype(F32)
    a_p = dot(ho, wo_o[1]).astype(BF16).astype(F32)
    c_wo.wait_recv()
    c_ho.wait_recv()
    hp = ho_p[...]
    a_o = a_o + dot(hp, wo_p[0]).astype(BF16).astype(F32)
    a_p = a_p + dot(hp, wo_p[1]).astype(BF16).astype(F32)
    after = (tok_f + a_o).astype(BF16).astype(F32)
    after_p = (tok_pf + a_p).astype(BF16).astype(F32)
    squares = jnp.sum(after * after, axis=1, keepdims=True) + jnp.sum(
        after_p * after_p, axis=1, keepdims=True
    )
    normed = (after * lax.rsqrt(squares / D + epsilon) * norm_ffn[...]).astype(BF16)

    chosen = dot(sel_m[:, :R].astype(BF16), normed).astype(BF16)
    xs[...] = chosen.astype(F32).reshape(EXPERTS, SLOT, H).astype(BF16)
    xe_d[0] = normed
    seat = {i: j for j, i in enumerate(NEAR)}
    z_far, z_near = Group(zr.at[pl.ds(3, 5)]), Group(zr.at[pl.ds(1, 2)])
    for i in PACKED[:-1]:
        group = z_far if i in PACKED[:5] else z_near
        group.add(xs.at[(z + i) % Z], zr.at[seat[Z - i]], zpeer[i])
    chunks = [Gather(buf) for buf in (xe_a, xe_b, xe_d)]
    chunks[2].start()
    gate_row = gate_vec[...].astype(F32)
    gate_row = jnp.concatenate([gate_row[r : r + 1] for r in range(H // 128)], axis=1)
    logit = jnp.sum(normed.astype(F32) * gate_row, axis=1, keepdims=True)
    lg_s[...] = logit + jnp.zeros((R, 128), F32)
    c_lg = remote(lg_s, lg_r, partner)
    def new_state(h):
        cols = slice(h * hs, (h + 1) * hs)
        for s in range(R):
            ns[s, h] = decays[h] * st[s, h] + k_t[cols, s : s + 1] * v[s : s + 1, cols]

    new_state(0)

    for name in ("eg", "eu", "ed"):
        local[name].wait()
    for copy in (c_eg, c_eu, c_ed):
        copy.wait_recv()
    for t in range(2):
        for src, dst in ((eg, w1.at[0, t]), (eu, w1.at[1, t]), (ed, w2.at[t])):
            dst[:FE] = src[t]
            dst[FE:] = jnp.zeros((128 - FE, H), BF16)
    weights.start()
    new_state(1)
    comb = [scl_m[(z + i) % Z] for i in NEAR]
    comb.append(jnp.zeros((128 - EXPERTS * SLOT, 128), F32))
    comb = jnp.concatenate(comb, axis=0).T[:R, : EXPERTS * SLOT].astype(BF16)

    xe, pe_o = (xe_a, xe_b, xe_d), (pe_o_a, pe_o_b, pe_o_d)
    pe_s, pe_r = (pe_s_a, pe_s_b, pe_s_d), (pe_r_a, pe_r_b, pe_r_d)
    y32, yb, rb = (y_a, y_b, y_d), (yb_a, yb_b, yb_d), (rb_a, rb_b, rb_d)
    sb, ra = (sb_a, sb_b, sb_d), (ra_a, ra_b, ra_d)
    enter = (w1, w1, w1d)
    leave = (w2, w2, w2d)

    def matches(shape, row_dim, blocks, start):
        row, slot = iota(shape, row_dim) + start, iota(shape, 1 - row_dim)
        found = jnp.zeros(shape, F32)
        for n, j in enumerate(blocks):
            hit = (slot - SLOT * n == row - CAP * j) & (row >= CAP * j) & (row < CAP * (j + 1))
            found = found + jnp.where(hit, 1.0, 0.0)
        return found.astype(BF16)

    def pack(c, blocks, start):
        parts = []
        for j in blocks:
            i = PACKED[j]
            parts.append((zr[seat[i]] if i else xs[z]).astype(F32))
        if len(parts) % 2:
            parts.append(jnp.zeros((SLOT, H), F32))
        rows = jnp.concatenate(parts, axis=0).astype(BF16)
        take = matches((CHUNKS[c], SLOT * len(parts)), 0, blocks, start)
        xe[c][0] = dot(take, rows).astype(BF16)
        chunks[c].start()

    z_far.wait_recv()
    pack(0, (0, 1, 2, 3, 4), 0)
    z_near.wait_recv()
    pack(1, (4, 5, 6, 7), CHUNKS[0])
    chunks[2].go()
    weights.start()
    chunks[0].go()
    chunks[1].go()
    weights.start()

    c_pe, c_rb, c_ra = {}, {}, {}

    def before_act(c):
        n = CHUNKS[c]
        chunks[c].across.wait_recv()
        pre = dot_t(xe[c][...].reshape(PLANE * n, H), enter[c][...].reshape(512, H))
        pe_o[c][...] = pre
        for b in range(SIDE):
            for a in range(SIDE):
                f = SIDE * b + a
                pe_s[c][SIDE * a + b] = pre[f * n : (f + 1) * n].astype(BF16)
        c_pe[c] = remote(pe_s[c], pe_r[c], partner)

    def act(c):
        n = CHUNKS[c]
        c_pe[c].wait_recv()
        pre = pe_o[c][...] + pe_r[c][...].astype(F32).reshape(PLANE * n, 512)
        hidden = (silu(pre[:, :256]) * pre[:, 256:]).astype(BF16)
        down = leave[c][...].reshape(256, H)
        gone = dot(hidden[SIDE * n :], down)
        yb[c][...] = gone.reshape(3 * SIDE, n, H).astype(BF16)
        c_rb[c] = Group(rb[c])
        for d, b in BACK:
            c_rb[c].add(yb[c].at[pl.ds(SIDE * (b - 1), SIDE)], rb[c].at[b - 1], second[d])
        y32[c][...] = dot(hidden[: SIDE * n], down).reshape(SIDE, n, H)

    def sum_second(c):
        c_rb[c].wait_recv()
        total = y32[c][...]
        for b in range(3):
            total = total + rb[c][b].astype(F32)
        sb[c][...] = total[1:].astype(BF16)
        c_ra[c] = Group(ra[c])
        for d, a in BACK:
            c_ra[c].add(sb[c].at[a - 1], ra[c].at[a - 1], first[d])
        y32[c][0] = total[0]

    c_ret = Group(zret.at[pl.ds(1, Z - 1)])

    def sum_first(c):
        c_ra[c].wait_recv()
        total = y32[c][0]
        for a in range(3):
            total = total + ra[c][a].astype(F32)
        return total

    def give_back(c, blocks):
        tot[sum(CHUNKS[:c]) : sum(CHUNKS[: c + 1])] = sum_first(c)
        done = tot[: sum(CHUNKS[: c + 1])]
        pad = -done.shape[0] % 16
        if pad:
            done = jnp.concatenate([done, jnp.zeros((pad, H), F32)], axis=0)
        put = matches((SLOT * len(blocks), done.shape[0]), 1, blocks, 0)
        rows = dot(put, done.astype(BF16))
        for n, j in enumerate(blocks):
            i = PACKED[j]
            block = rows[n * SLOT : (n + 1) * SLOT].astype(BF16)
            if i == 0:
                zret[0] = block
            else:
                zs[i] = block
                c_ret.add(zs.at[i], zret.at[seat[Z - i]], zpeer[i])

    before_act(0)
    act(0)
    before_act(1)
    weights.start()
    for j in range(Z):
        for t, dst in enumerate((w1d.at[0, j], w1d.at[1, j], w2d.at[j])):
            dst[:FD] = wbuf[j, t]
            dst[FD:] = jnp.zeros((32 - FD, H), BF16)
    before_act(2)
    act(1)
    sum_second(0)
    act(2)
    give_back(0, (0, 1, 2, 3))
    sum_second(1)
    sum_second(2)
    give_back(1, (4, 5, 6, 7))
    dense = sum_first(2)

    c_lg.wait_recv()
    open_ = 1.0 / (1.0 + jnp.exp(-(lg_s[:, :1] + lg_r[:, :1])))
    c_ret.wait_recv()
    back = zret[...].astype(F32).reshape(EXPERTS * SLOT, H).astype(BF16)
    moe = dot(comb, back)
    mixed[...] = (after + moe + open_ * dense).astype(BF16)
    for group in sent:
        group.wait_send()
    assert (len(sent), len(local)) == (GROUPS, LOADS), (len(sent), len(local))


def store(a_in, b_in, a_out, b_out, sems):
    first = pltpu.make_async_copy(b_in, b_out, sems.at[0])
    second = pltpu.make_async_copy(a_in, a_out, sems.at[1])
    first.start()
    second.start()
    first.wait()
    second.wait()


def body(
    tokens,
    state,
    norm_mix,
    w_query,
    w_key,
    w_value,
    w_out,
    norm_ffn,
    gate_vector,
    dense_gate,
    dense_up,
    dense_down,
    exp_gate,
    exp_up,
    exp_down,
    routes,
    route_w,
):
    R, H = tokens.shape
    heads, hs = state.shape[1], state.shape[2]
    HW = heads * hs
    FE = exp_gate.shape[2]
    FD = dense_gate.shape[1]
    Z = EXPERTS
    per_chunk = lambda make: [make(n) for n in CHUNKS]
    vm = pl.BlockSpec(memory_space=pltpu.VMEM)
    hbm = pl.BlockSpec(memory_space=pltpu.HBM)
    V = pltpu.VMEM
    sem = lambda *shape: pltpu.SemaphoreType.DMA(shape)
    operands = (
        tokens,
        norm_mix.reshape(1, -1),
        routes.T,
        route_w.T,
        norm_ffn.reshape(1, -1),
        gate_vector.reshape(-1, 128),
        state,
        w_query,
        w_key,
        w_value,
        w_out,
        dense_gate.T,
        dense_up.T,
        dense_down,
        exp_gate[0].T,
        exp_up[0].T,
        exp_down,
    )
    held = [pltpu.with_memory_space_constraint(x, pltpu.HBM) for x in operands]
    mixed, new_state = pl.pallas_call(
        kernel,
        out_shape=(pltpu.VMEM((R, H), BF16), pltpu.VMEM(state.shape, F32)),
        in_specs=[hbm] * 17,
        out_specs=(vm, vm),
        scratch_shapes=[
            V((R, H), BF16),
            V((1, 2 * H), F32),
            V((routes.shape[1], R), jnp.int32),
            V((routes.shape[1], R), BF16),
            V((1, H), F32),
            V((H // 128, 128), BF16),
            V((R, H), BF16),
            V((2, H, HW), BF16),
            V((2, H, HW), BF16),
            V((2, H, HW), BF16),
            V((2, HW, H), BF16),
            V((2, HW, H), BF16),
            V((2, FE, H), BF16),
            V((2, FE, H), BF16),
            V((2, FE, H), BF16),
            V(state.shape, F32),
            V((R, HW), BF16),
            V((R, HW), BF16),
            V((EXPERTS * SLOT, 128), F32),
            V((EXPERTS, SLOT, 128), F32),
            V((R, 128), F32),
            V((R, 128), F32),
            V((Z, 3, FD, H), BF16),
            V((2, 2, 128, H), BF16),
            V((2, 128, H), BF16),
            V((2, Z, 32, H), BF16),
            V((Z, 32, H), BF16),
            V((EXPERTS, SLOT, H), BF16),
            V((Z, SLOT, H), BF16),
            *per_chunk(lambda n: V((PLANE, n, H), BF16)),
            *per_chunk(lambda n: V((PLANE * n, 512), F32)),
            *per_chunk(lambda n: V((PLANE, n, 512), BF16)),
            *per_chunk(lambda n: V((PLANE, n, 512), BF16)),
            *per_chunk(lambda n: V((SIDE, n, H), F32)),
            *per_chunk(lambda n: V((3 * SIDE, n, H), BF16)),
            *per_chunk(lambda n: V((3, SIDE, n, H), BF16)),
            *per_chunk(lambda n: V((3, n, H), BF16)),
            *per_chunk(lambda n: V((3, n, H), BF16)),
            V((sum(CHUNKS[:2]), H), F32),
            V((Z, SLOT, H), BF16),
            V((Z, SLOT, H), BF16),
            sem(LOADS),
            sem(GROUPS),
            sem(GROUPS),
        ],
        compiler_params=pltpu.CompilerParams(
            collective_id=0, has_side_effects=True, vmem_limit_bytes=50 * 1024 * 1024
        ),
        name="layer",
    )(
        *held
    )
    return pl.pallas_call(
        store,
        out_shape=(
            jax.ShapeDtypeStruct((R, H), BF16),
            jax.ShapeDtypeStruct(state.shape, F32),
        ),
        in_specs=[vm, vm],
        out_specs=(hbm, hbm),
        scratch_shapes=[sem(2)],
        name="store",
    )(
        pltpu.with_memory_space_constraint(mixed, pltpu.VMEM),
        pltpu.with_memory_space_constraint(new_state, pltpu.VMEM),
    )


def solution(mesh):
    return jax.shard_map(
        body,
        mesh=mesh,
        in_specs=(
            P("ep", "tp"),
            P("ep", "tp", None, None),
            P(),
            P(None, "tp"),
            P(None, "tp"),
            P(None, "tp"),
            P("tp", None),
            P("tp"),
            P("tp"),
            P("tp", "ep"),
            P("tp", "ep"),
            P("ep", "tp"),
            P("ep", None, "tp"),
            P("ep", None, "tp"),
            P("ep", "tp", None),
            P("ep", None),
            P("ep", None),
        ),
        out_specs=(P("ep", "tp"), P("ep", "tp", None, None)),
        check_vma=False,
    )
```

```python
import functools

import jax
import jax.numpy as jnp
from jax import lax
from jax.experimental import pallas as pl
from jax.experimental.pallas import tpu as pltpu
from jax.sharding import PartitionSpec as P

EXPERTS = 8
CAP = 5
SLOT = 8
SIDE = 4
PLANE = SIDE * SIDE
NEAR = (0, 1, 7, 2, 6, 3, 5, 4)
TRIPS = (
    ((1, 0, CAP), (2, 0, CAP), (6, 0, CAP), (7, 0, 1)),
    ((3, 0, CAP), (4, 0, CAP), (5, 0, CAP), (7, 1, 1)),
    ((7, 2, CAP - 2), (0, 0, CAP)),
)
CHUNKS = (16, 16, 8, 16)
DENSE = len(CHUNKS) - 1
RELAY_IN = ()
RELAY_OUT = ()
GROUPS = 38 + len(RELAY_IN) + len(RELAY_OUT)
LOADS = 21
epsilon = 1e-06
MESH = pl.DeviceIdType.MESH
F32 = jnp.float32
BF16 = jnp.bfloat16


def dot(a, b):
    return jnp.dot(a, b, preferred_element_type=F32)


def dot_t(a, b):
    return lax.dot_general(a, b, (((1,), (1,)), ((), ())), preferred_element_type=F32)


def silu(v):
    return v / (1.0 + jnp.exp(-v))


def iota(shape, dim):
    return lax.broadcasted_iota(jnp.int32, shape, dim)


def kernel(
    tokens_h,
    norm_mix_h,
    routes_h,
    route_w_h,
    norm_ffn_h,
    gate_vec_h,
    state,
    w_query,
    w_key,
    w_value,
    w_out,
    dense_gate,
    dense_up,
    dense_down,
    exp_gate,
    exp_up,
    exp_down,
    mixed,
    ns,
    tokens,
    norm_mix,
    routes,
    route_w,
    norm_ffn,
    gate_vec,
    tok_p,
    wq,
    wk,
    wv,
    wo_o,
    wo_p,
    eg,
    eu,
    ed,
    st,
    ho_o,
    ho_p,
    sel_m,
    scl_m,
    lg_s,
    lg_r,
    wbuf,
    w1,
    w2,
    w1d,
    w2d,
    xs,
    zr,
    xe_a,
    xe_b,
    xe_c,
    xe_d,
    pe_o_a,
    pe_o_b,
    pe_o_c,
    pe_o_d,
    pe_s_a,
    pe_s_b,
    pe_s_c,
    pe_s_d,
    pe_r_a,
    pe_r_b,
    pe_r_c,
    pe_r_d,
    y_a,
    y_b,
    y_c,
    y_d,
    yb_a,
    yb_b,
    yb_c,
    yb_d,
    rb_a,
    rb_b,
    rb_c,
    rb_d,
    sb_a,
    sb_b,
    sb_c,
    sb_d,
    ra_a,
    ra_b,
    ra_c,
    ra_d,
    tot,
    zs,
    zret,
    lsem,
    ssem,
    rsem,
):
    R, H = tokens.shape
    D = 2 * H
    heads, hs = state.shape[1], state.shape[2]
    HW = heads * hs
    FE = eg.shape[1]
    FD = wbuf.shape[2]
    Z = EXPERTS
    me = lax.axis_index("ep")
    tp = lax.axis_index("tp")
    other = 1 - tp
    z, y_at, x_at = me // PLANE, (me // SIDE) % SIDE, me % SIDE

    def in_plane(dy, dx):
        return {
            "ep": z * PLANE + ((y_at + dy + SIDE) % SIDE) * SIDE + (x_at + dx + SIDE) % SIDE,
            "tp": tp,
        }

    first = {d: in_plane(tp * d, other * d) for d in (1, -1, 2)}
    second = {d: in_plane(other * d, tp * d) for d in (1, -1, 2)}
    zpeer = [{"ep": ((z + i) % Z) * PLANE + me % PLANE, "tp": tp} for i in range(Z)]
    partner = {"ep": me, "tp": other}

    own = pl.ds(pl.multiple_of(tp * H, H), H)
    oth = pl.ds(pl.multiple_of(other * H, H), H)

    sent = []

    class Group:
        def __init__(self, whole):
            self.k, self.whole = len(sent), whole
            sent.append(self)

        def copy(self, src, dst, dev):
            self.dev = dev
            return pltpu.make_async_remote_copy(
                src_ref=src,
                dst_ref=dst,
                send_sem=ssem.at[self.k],
                recv_sem=rsem.at[self.k],
                device_id=dev,
                device_id_type=MESH,
            )

        def add(self, src, dst, dev):
            self.copy(src, dst, dev).start()

        def wait_recv(self):
            self.copy(self.whole, self.whole, self.dev).wait_recv()

        def wait_send(self):
            self.copy(self.whole, self.whole, self.dev).wait_send()

    def remote(src, dst, dev):
        group = Group(dst)
        group.add(src, dst, dev)
        return group

    local = {}

    def load(name, src, dst):
        copy = pltpu.make_async_copy(src, dst, lsem.at[len(local)])
        copy.start()
        local[name] = copy

    HOPS = ((1, 1), (-1, 2), (2, 3))
    BACK = ((2, 3), (-1, 1), (1, 2))

    class Gather:
        def __init__(self, buf, relayed):
            self.at, self.relayed = buf.at, relayed

        def spread(self, *todo):
            for d, b in HOPS[:2] if self.relayed else HOPS:
                for a in todo:
                    self.across.add(self.at[a], self.at[SIDE * b + a], second[d])

        def start(self):
            at = self.at
            self.near, self.far = Group(at[pl.ds(1, 2)]), Group(at[3])
            self.across = Group(at[pl.ds(SIDE, (2 if self.relayed else 3) * SIDE)])
            self.near.add(at[0], at[1], first[1])
            self.near.add(at[0], at[2], first[-1])
            self.far.add(at[0], at[3], first[2])

        def go(self):
            self.near.wait_recv()
            self.spread(1, 2)
            self.far.wait_recv()
            self.spread(3)

        def relay(self):
            at = self.at
            self.across.wait_recv()
            self.across = Group(at[pl.ds(3 * SIDE, SIDE)])
            for a, b, d in ((0, 1, 1), (1, 1, 1), (2, 2, -1), (3, 2, -1)):
                self.across.add(at[SIDE * b + a], at[3 * SIDE + a], second[d])

    class Ring:
        def __init__(self, buf):
            self.at, self.step = buf.at, 0

        def start(self):
            at, t = self.at, self.step
            if t:
                self.group.wait_recv()
            up, down = max(0, 2 * t), max(0, 2 * t - 1)
            if t < 3:
                self.group = Group(at[pl.ds(2 * t + 1, 2)])
                self.group.add(at[up], at[2 * t + 2], zpeer[1])
                self.group.add(at[down], at[2 * t + 1], zpeer[-1])
            elif t == 3:
                self.group = Group(at[7])
                self.group.add(at[up, pl.ds(0, 2)], at[7, pl.ds(0, 2)], zpeer[1])
                self.group.add(at[down, pl.ds(2, 1)], at[7, pl.ds(2, 1)], zpeer[-1])
            self.step = t + 1

    small = (
        (tokens_h, tokens),
        (norm_mix_h, norm_mix),
        (routes_h, routes),
        (route_w_h, route_w),
        (norm_ffn_h, norm_ffn),
        (gate_vec_h, gate_vec),
    )
    barrier = pltpu.get_barrier_semaphore()
    greeted = [partner, *first.values(), *second.values()] + zpeer[1:]
    for dev in greeted:
        pl.semaphore_signal(barrier, inc=1, device_id=dev, device_id_type=MESH)

    for t, (src, dst) in enumerate(small):
        load(f"s{t}", src, dst)
    for t, src in enumerate((dense_gate, dense_up, dense_down)):
        load(f"d{t}", src, wbuf.at[0, t])
    for t, (src, dst) in enumerate(((w_query, wq), (w_key, wk), (w_value, wv))):
        load(f"p{t}o", src.at[own, :], dst.at[0])
        load(f"p{t}p", src.at[oth, :], dst.at[1])
    load("st", state, st)
    load("wo0", w_out.at[:, own], wo_o.at[0])
    load("wo1", w_out.at[:, oth], wo_o.at[1])
    load("eg", exp_gate.at[:, own], eg.at[tp])
    load("eu", exp_up.at[:, own], eu.at[tp])
    load("ed", exp_down.at[0, :, own], ed.at[tp])

    local["s0"].wait()
    pl.semaphore_wait(barrier, len(greeted))

    c_tok = remote(tokens, tok_p, partner)
    weights = Ring(wbuf)
    for t in range(3):
        local[f"d{t}"].wait()
    weights.start()
    c_wo = Group(wo_p)
    c_wo.add(w_out.at[:, oth], wo_p.at[0], partner)
    c_wo.add(w_out.at[:, own], wo_p.at[1], partner)
    c_eg = remote(exp_gate.at[:, oth], eg.at[tp], partner)
    c_eu = remote(exp_up.at[:, oth], eu.at[tp], partner)
    c_ed = remote(exp_down.at[0, :, oth], ed.at[tp], partner)

    for t in (2, 3):
        local[f"s{t}"].wait()
    row_id = iota((EXPERTS, R), 0)
    wt = jnp.zeros((EXPERTS, R), F32)
    member = jnp.zeros((EXPERTS, R), F32)
    named = routes[...]
    gains = route_w[...].astype(F32)
    for t in range(routes.shape[0]):
        hit = row_id == named[t : t + 1, :]
        wt = wt + jnp.where(hit, gains[t : t + 1, :], 0.0)
        member = member + jnp.where(hit, 1.0, 0.0)
    blank = jnp.zeros((EXPERTS, 128 - R), F32)
    wt = jnp.concatenate([wt, blank], axis=1)
    member = jnp.concatenate([member, blank], axis=1)
    before = jnp.where(iota((128, 128), 0) < iota((128, 128), 1), 1.0, 0.0).astype(BF16)
    rank = dot(member.astype(BF16), before)
    slot_id = iota((SLOT, 128), 0).astype(F32)
    picks = []
    for e in range(EXPERTS):
        pick = jnp.where(rank[e : e + 1] == slot_id, member[e : e + 1], 0.0)
        picks.append(pick)
        scl_m[e] = pick * wt[e : e + 1]
    sel_m[...] = jnp.concatenate(picks, axis=0)
    for t in (1, 4, 5):
        local[f"s{t}"].wait()

    tok_f = tokens[...].astype(F32)
    c_tok.wait_recv()
    tok_pf = tok_p[...].astype(F32)
    total = jnp.sum(tok_f * tok_f, axis=1, keepdims=True) + jnp.sum(
        tok_pf * tok_pf, axis=1, keepdims=True
    )
    scale = lax.rsqrt(total / D + epsilon)
    gain_o = norm_mix[:, own]
    gain_p = norm_mix[:, oth]
    nx_o = (tok_f * scale * gain_o).astype(BF16)
    nx_p = (tok_pf * scale * gain_p).astype(BF16)
    proj = []
    for t, w in enumerate((wq, wk, wv)):
        local[f"p{t}o"].wait()
        part = dot(nx_o, w[0])
        local[f"p{t}p"].wait()
        proj.append((part + dot(nx_p, w[1])).astype(BF16).astype(F32))
    q, k, v = proj
    k = k * hs ** (-0.5)
    pad = jnp.zeros((128 - R, HW), F32)
    q_t = jnp.concatenate([q, pad], axis=0).T
    k_t = jnp.concatenate([k, pad], axis=0).T
    head_id = tp * heads
    local["st"].wait()
    decays = []
    for h in range(heads):
        cols = slice(h * hs, (h + 1) * hs)
        idv = jnp.zeros((1, 128), F32) + (head_id + h).astype(F32)
        decay = 1.0 - jnp.exp2(-3.0 - 2.0 * idv)
        decays.append(decay)
        rows = []
        for s in range(R):
            rows.append(jnp.sum(st[s, h] * q_t[cols, s : s + 1], axis=0, keepdims=True))
        qs = jnp.concatenate(rows, axis=0)
        qk = jnp.sum(q[:, cols] * k[:, cols], axis=1, keepdims=True)
        read = decay * qs + qk * v[:, cols]
        centre = jnp.mean(read, axis=1, keepdims=True)
        dev = read - centre
        spread = jnp.mean(dev * dev, axis=1, keepdims=True)
        ho_o[:, cols] = (dev * lax.rsqrt(spread + epsilon)).astype(BF16)
    c_ho = remote(ho_o, ho_p, partner)
    ho = ho_o[...]
    local["wo0"].wait()
    local["wo1"].wait()
    a_o = dot(ho, wo_o[0]).astype(BF16).astype(F32)
    a_p = dot(ho, wo_o[1]).astype(BF16).astype(F32)
    c_wo.wait_recv()
    c_ho.wait_recv()
    hp = ho_p[...]
    a_o = a_o + dot(hp, wo_p[0]).astype(BF16).astype(F32)
    a_p = a_p + dot(hp, wo_p[1]).astype(BF16).astype(F32)
    after = (tok_f + a_o).astype(BF16).astype(F32)
    after_p = (tok_pf + a_p).astype(BF16).astype(F32)
    squares = jnp.sum(after * after, axis=1, keepdims=True) + jnp.sum(
        after_p * after_p, axis=1, keepdims=True
    )
    normed = (after * lax.rsqrt(squares / D + epsilon) * norm_ffn[...]).astype(BF16)

    chosen = dot(sel_m[:, :R].astype(BF16), normed).astype(BF16)
    xs[...] = chosen.astype(F32).reshape(EXPERTS, SLOT, H).astype(BF16)
    xe_d[0] = normed
    seat = {i: j for j, i in enumerate(NEAR)}
    z_near, z_far = Group(zr.at[pl.ds(1, 4)]), Group(zr.at[pl.ds(5, 3)])
    for i in (2, 6, 1, 7, 4, 3, 5):
        group = z_near if i in NEAR[:5] else z_far
        group.add(xs.at[(z + i) % Z], zr.at[seat[Z - i]], zpeer[i])
    xe = (xe_a, xe_b, xe_c, xe_d)
    chunks = [Gather(buf, c in RELAY_IN) for c, buf in enumerate(xe)]
    chunks[DENSE].start()
    chunks[DENSE].spread(0)
    gate_row = gate_vec[...].astype(F32)
    gate_row = jnp.concatenate([gate_row[r : r + 1] for r in range(H // 128)], axis=1)
    logit = jnp.sum(normed.astype(F32) * gate_row, axis=1, keepdims=True)
    lg_s[...] = logit + jnp.zeros((R, 128), F32)
    c_lg = remote(lg_s, lg_r, partner)
    def new_state(h):
        cols = slice(h * hs, (h + 1) * hs)
        for s in range(R):
            ns[s, h] = decays[h] * st[s, h] + k_t[cols, s : s + 1] * v[s : s + 1, cols]

    new_state(0)

    for name in ("eg", "eu", "ed"):
        local[name].wait()
    for copy in (c_eg, c_eu, c_ed):
        copy.wait_recv()
    for t in range(2):
        for src, dst in ((eg, w1.at[0, t]), (eu, w1.at[1, t]), (ed, w2.at[t])):
            dst[:FE] = src[t]
            dst[FE:] = jnp.zeros((128 - FE, H), BF16)
    new_state(1)
    comb = [scl_m[(z + i) % Z] for i in NEAR]
    comb.append(jnp.zeros((128 - EXPERTS * SLOT, 128), F32))
    comb = jnp.concatenate(comb, axis=0).T[:R, : EXPERTS * SLOT].astype(BF16)

    pe_o = (pe_o_a, pe_o_b, pe_o_c, pe_o_d)
    pe_s = (pe_s_a, pe_s_b, pe_s_c, pe_s_d)
    pe_r = (pe_r_a, pe_r_b, pe_r_c, pe_r_d)
    y32, yb = (y_a, y_b, y_c, y_d), (yb_a, yb_b, yb_c, yb_d)
    rb, sb = (rb_a, rb_b, rb_c, rb_d), (sb_a, sb_b, sb_c, sb_d)
    ra = (ra_a, ra_b, ra_c, ra_d)
    enter = (w1, w1, w1, w1d)
    leave = (w2, w2, w2, w2d)

    def matches(shape, row_dim, order, trips):
        row, slot = iota(shape, row_dim), iota(shape, 1 - row_dim)
        found, first_row = jnp.zeros(shape, F32), 0
        for i, first_slot, count in trips:
            if i in order:
                shift = SLOT * order.index(i) + first_slot - first_row
                hit = (slot - row == shift) & (row >= first_row) & (row < first_row + count)
                found = found + jnp.where(hit, 1.0, 0.0)
            first_row += count
        return found.astype(BF16)

    def pack(c):
        order = [i for i, _, _ in TRIPS[c]]
        parts = [(zr[seat[i]] if i else xs[z]).astype(F32) for i in order]
        if len(parts) % 2:
            parts.append(jnp.zeros((SLOT, H), F32))
        rows = jnp.concatenate(parts, axis=0).astype(BF16)
        take = matches((CHUNKS[c], SLOT * len(parts)), 0, order, TRIPS[c])
        xe[c][0] = dot(take, rows).astype(BF16)
        chunks[c].start()

    z_near.wait_recv()
    pack(0)
    pack(2)
    chunks[0].spread(0)
    chunks[2].spread(0)
    weights.start()
    chunks[DENSE].go()
    z_far.wait_recv()
    pack(1)
    chunks[1].spread(0)
    chunks[0].go()
    chunks[2].go()
    weights.start()
    chunks[1].go()

    c_pe, c_rx, c_rb, c_ra = {}, {}, {}, {}

    def before_act(c):
        n = CHUNKS[c]
        chunks[c].across.wait_recv()
        pre = dot_t(xe[c][...].reshape(PLANE * n, H), enter[c][...].reshape(512, H))
        pe_o[c][...] = pre
        for b in range(SIDE):
            for a in range(SIDE):
                f = SIDE * b + a
                pe_s[c][SIDE * a + b] = pre[f * n : (f + 1) * n].astype(BF16)
        c_pe[c] = remote(pe_s[c], pe_r[c], partner)

    def act(c):
        n = CHUNKS[c]
        c_pe[c].wait_recv()
        pre = pe_o[c][...] + pe_r[c][...].astype(F32).reshape(PLANE * n, 512)
        hidden = (silu(pre[:, :256]) * pre[:, 256:]).astype(BF16)
        down = leave[c][...].reshape(256, H)
        gone = dot(hidden[SIDE * n :], down)
        yb[c][...] = gone.reshape(3 * SIDE, n, H).astype(BF16)
        out, at = yb[c].at, rb[c].at
        if c in RELAY_OUT:
            low, high = pl.ds(0, 2), pl.ds(2, 2)
            c_rx[c] = Group(at[2])
            c_rx[c].add(out[pl.ds(2 * SIDE, 2)], at[2, low], second[1])
            c_rx[c].add(out[pl.ds(2 * SIDE + 2, 2)], at[2, high], second[-1])
            c_rb[c] = Group(at[pl.ds(0, 2)])
            c_rb[c].add(out[pl.ds(SIDE + 2, 2)], at[0, high], second[1])
            c_rb[c].add(out[low], at[1, low], second[-1])
        else:
            c_rb[c] = Group(rb[c])
            for d, b in BACK:
                c_rb[c].add(out[pl.ds(SIDE * (b - 1), SIDE)], at[b - 1], second[d])
        y32[c][...] = dot(hidden[: SIDE * n], down).reshape(SIDE, n, H)

    def sum_relay(c):
        c_rx[c].wait_recv()
        n, out, at = CHUNKS[c], yb[c], rb[c].at
        for half, slot, d in ((0, SIDE, 1), (1, 2, -1)):
            here, part = pl.ds(slot, 2), pl.ds(2 * half, 2)
            more = out[slot : slot + 2].astype(F32) + rb[c][2, 2 * half : 2 * half + 2].astype(F32)
            out[slot : slot + 2] = more.astype(BF16)
            c_rb[c].add(out.at[here], at[half, part], second[d])

    def sum_second(c):
        c_rb[c].wait_recv()
        total = y32[c][...]
        for b in range(2 if c in RELAY_OUT else 3):
            total = total + rb[c][b].astype(F32)
        sb[c][...] = total[1:].astype(BF16)
        c_ra[c] = Group(ra[c])
        for d, a in BACK:
            c_ra[c].add(sb[c].at[a - 1], ra[c].at[a - 1], first[d])
        y32[c][0] = total[0]

    c_ret = Group(zret.at[pl.ds(1, Z - 1)])

    def sum_first(c):
        c_ra[c].wait_recv()
        total = y32[c][0]
        for a in range(3):
            total = total + ra[c][a].astype(F32)
        return total

    def give_back(c, *order):
        tot[sum(CHUNKS[:c]) : sum(CHUNKS[: c + 1])] = sum_first(c)
        done = tot[: sum(CHUNKS[: c + 1])]
        pad = -done.shape[0] % 16
        if pad:
            done = jnp.concatenate([done, jnp.zeros((pad, H), F32)], axis=0)
        put = matches((SLOT * len(order), done.shape[0]), 1, order, sum(TRIPS[: c + 1], ()))
        rows = dot(put, done.astype(BF16))
        for n, i in enumerate(order):
            block = rows[n * SLOT : (n + 1) * SLOT].astype(BF16)
            if i == 0:
                zret[0] = block
            else:
                zs[i] = block
                c_ret.add(zs.at[i], zret.at[seat[Z - i]], zpeer[i])

    before_act(0)
    weights.start()
    act(0)
    before_act(1)
    before_act(2)
    act(1)
    weights.start()
    for j in range(Z):
        for t, dst in enumerate((w1d.at[0, j], w1d.at[1, j], w2d.at[j])):
            dst[:FD] = wbuf[j, t]
            dst[FD:] = jnp.zeros((32 - FD, H), BF16)
    before_act(DENSE)
    act(2)
    sum_second(0)
    act(DENSE)
    sum_second(1)
    give_back(0, 1, 2, 6)
    sum_second(2)
    give_back(1, 3, 4, 5)
    sum_second(DENSE)
    give_back(2, 7, 0)
    dense = sum_first(DENSE)

    c_lg.wait_recv()
    open_ = 1.0 / (1.0 + jnp.exp(-(lg_s[:, :1] + lg_r[:, :1])))
    c_ret.wait_recv()
    back = zret[...].astype(F32).reshape(EXPERTS * SLOT, H).astype(BF16)
    moe = dot(comb, back)
    mixed[...] = (after + moe + open_ * dense).astype(BF16)
    for group in sent:
        group.wait_send()
    assert (len(sent), len(local)) == (GROUPS, LOADS), (len(sent), len(local))


def store(a_in, b_in, a_out, b_out, sems):
    first = pltpu.make_async_copy(b_in, b_out, sems.at[0])
    second = pltpu.make_async_copy(a_in, a_out, sems.at[1])
    first.start()
    second.start()
    first.wait()
    second.wait()


def body(
    tokens,
    state,
    norm_mix,
    w_query,
    w_key,
    w_value,
    w_out,
    norm_ffn,
    gate_vector,
    dense_gate,
    dense_up,
    dense_down,
    exp_gate,
    exp_up,
    exp_down,
    routes,
    route_w,
):
    R, H = tokens.shape
    heads, hs = state.shape[1], state.shape[2]
    HW = heads * hs
    FE = exp_gate.shape[2]
    FD = dense_gate.shape[1]
    Z = EXPERTS
    per_chunk = lambda make: [make(n) for n in CHUNKS]
    vm = pl.BlockSpec(memory_space=pltpu.VMEM)
    hbm = pl.BlockSpec(memory_space=pltpu.HBM)
    V = pltpu.VMEM
    sem = lambda *shape: pltpu.SemaphoreType.DMA(shape)
    operands = (
        tokens,
        norm_mix.reshape(1, -1),
        routes.T,
        route_w.T,
        norm_ffn.reshape(1, -1),
        gate_vector.reshape(-1, 128),
        state,
        w_query,
        w_key,
        w_value,
        w_out,
        dense_gate.T,
        dense_up.T,
        dense_down,
        exp_gate[0].T,
        exp_up[0].T,
        exp_down,
    )
    held = [pltpu.with_memory_space_constraint(x, pltpu.HBM) for x in operands]
    mixed, new_state = pl.pallas_call(
        kernel,
        out_shape=(pltpu.VMEM((R, H), BF16), pltpu.VMEM(state.shape, F32)),
        in_specs=[hbm] * 17,
        out_specs=(vm, vm),
        scratch_shapes=[
            V((R, H), BF16),
            V((1, 2 * H), F32),
            V((routes.shape[1], R), jnp.int32),
            V((routes.shape[1], R), BF16),
            V((1, H), F32),
            V((H // 128, 128), BF16),
            V((R, H), BF16),
            V((2, H, HW), BF16),
            V((2, H, HW), BF16),
            V((2, H, HW), BF16),
            V((2, HW, H), BF16),
            V((2, HW, H), BF16),
            V((2, FE, H), BF16),
            V((2, FE, H), BF16),
            V((2, FE, H), BF16),
            V(state.shape, F32),
            V((R, HW), BF16),
            V((R, HW), BF16),
            V((EXPERTS * SLOT, 128), F32),
            V((EXPERTS, SLOT, 128), F32),
            V((R, 128), F32),
            V((R, 128), F32),
            V((Z, 3, FD, H), BF16),
            V((2, 2, 128, H), BF16),
            V((2, 128, H), BF16),
            V((2, Z, 32, H), BF16),
            V((Z, 32, H), BF16),
            V((EXPERTS, SLOT, H), BF16),
            V((Z, SLOT, H), BF16),
            *per_chunk(lambda n: V((PLANE, n, H), BF16)),
            *per_chunk(lambda n: V((PLANE * n, 512), F32)),
            *per_chunk(lambda n: V((PLANE, n, 512), BF16)),
            *per_chunk(lambda n: V((PLANE, n, 512), BF16)),
            *per_chunk(lambda n: V((SIDE, n, H), F32)),
            *per_chunk(lambda n: V((3 * SIDE, n, H), BF16)),
            *per_chunk(lambda n: V((3, SIDE, n, H), BF16)),
            *per_chunk(lambda n: V((3, n, H), BF16)),
            *per_chunk(lambda n: V((3, n, H), BF16)),
            V((sum(CHUNKS[:DENSE]), H), F32),
            V((Z, SLOT, H), BF16),
            V((Z, SLOT, H), BF16),
            sem(LOADS),
            sem(GROUPS),
            sem(GROUPS),
        ],
        compiler_params=pltpu.CompilerParams(
            collective_id=0, has_side_effects=True, vmem_limit_bytes=50 * 1024 * 1024
        ),
        name="layer",
    )(
        *held
    )
    return pl.pallas_call(
        store,
        out_shape=(
            jax.ShapeDtypeStruct((R, H), BF16),
            jax.ShapeDtypeStruct(state.shape, F32),
        ),
        in_specs=[vm, vm],
        out_specs=(hbm, hbm),
        scratch_shapes=[sem(2)],
        name="store",
    )(
        pltpu.with_memory_space_constraint(mixed, pltpu.VMEM),
        pltpu.with_memory_space_constraint(new_state, pltpu.VMEM),
    )


def solution(mesh):
    return jax.shard_map(
        body,
        mesh=mesh,
        in_specs=(
            P("ep", "tp"),
            P("ep", "tp", None, None),
            P(),
            P(None, "tp"),
            P(None, "tp"),
            P(None, "tp"),
            P("tp", None),
            P("tp"),
            P("tp"),
            P("tp", "ep"),
            P("tp", "ep"),
            P("ep", "tp"),
            P("ep", None, "tp"),
            P("ep", None, "tp"),
            P("ep", "tp", None),
            P("ep", None),
            P("ep", None),
        ),
        out_specs=(P("ep", "tp"), P("ep", "tp", None, None)),
        check_vma=False,
    )
```

```python
import functools

import jax
import jax.numpy as jnp
from jax import lax
from jax.experimental import pallas as pl
from jax.experimental.pallas import tpu as pltpu
from jax.sharding import PartitionSpec as P

EXPERTS = 8
CAP = 5
SLOT = 8
SIDE = 4
PLANE = SIDE * SIDE
NEAR = (0, 1, 7, 2, 6, 3, 5, 4)
TRIPS = (
    ((1, 0, CAP), (2, 0, CAP), (6, 0, CAP), (7, 0, 1)),
    ((3, 0, CAP), (4, 0, CAP), (5, 0, CAP), (7, 1, 1)),
    ((7, 2, CAP - 2), (0, 0, CAP)),
)
CHUNKS = (16, 16, 8, 16)
DENSE = len(CHUNKS) - 1
GROUPS = 36
SENDS = 24
LOADS = 17
epsilon = 1e-06
MESH = pl.DeviceIdType.MESH
F32 = jnp.float32
BF16 = jnp.bfloat16


def dot(a, b):
    return jnp.dot(a, b, preferred_element_type=F32)


def dot_t(a, b):
    return lax.dot_general(a, b, (((1,), (1,)), ((), ())), preferred_element_type=F32)


def silu(v):
    return v / (1.0 + jnp.exp(-v))


def iota(shape, dim):
    return lax.broadcasted_iota(jnp.int32, shape, dim)


def kernel(
    tokens_h,
    norm_mix_h,
    routes_h,
    route_w_h,
    norm_ffn_h,
    gate_vec_h,
    state,
    w_query,
    w_key,
    w_value,
    w_out,
    dense_gate,
    dense_up,
    dense_down,
    exp_gate,
    exp_up,
    exp_down,
    mixed,
    ns,
    tokens,
    norm_mix,
    routes,
    route_w,
    norm_ffn,
    gate_vec,
    tok_p,
    wq,
    wk,
    wv,
    wo_o,
    wo_p,
    we,
    st,
    ho_o,
    ho_p,
    sel_m,
    scl_m,
    lg_s,
    lg_r,
    wbuf,
    w1,
    w2,
    w1d,
    w2d,
    xs,
    zr,
    xe_a,
    xe_b,
    xe_c,
    xe_d,
    pe_o_a,
    pe_o_b,
    pe_o_c,
    pe_o_d,
    pe_s_a,
    pe_s_b,
    pe_s_c,
    pe_s_d,
    pe_r_a,
    pe_r_b,
    pe_r_c,
    pe_r_d,
    y_a,
    y_b,
    y_c,
    y_d,
    yb_a,
    yb_b,
    yb_c,
    yb_d,
    rb_a,
    rb_b,
    rb_c,
    rb_d,
    sb_a,
    sb_b,
    sb_c,
    sb_d,
    ra_a,
    ra_b,
    ra_c,
    ra_d,
    tot,
    zs,
    zret,
    lsem,
    ssem,
    rsem,
    gsem,
):
    R, H = tokens.shape
    D = 2 * H
    heads, hs = state.shape[1], state.shape[2]
    HW = heads * hs
    FE = we.shape[2]
    FD = wbuf.shape[2]
    Z = EXPERTS
    me = lax.axis_index("ep")
    tp = lax.axis_index("tp")
    other = 1 - tp
    z, y_at, x_at = me // PLANE, (me // SIDE) % SIDE, me % SIDE

    def in_plane(dy, dx):
        return {
            "ep": z * PLANE + ((y_at + dy + SIDE) % SIDE) * SIDE + (x_at + dx + SIDE) % SIDE,
            "tp": tp,
        }

    first = {d: in_plane(tp * d, other * d) for d in (1, -1, 2)}
    second = {d: in_plane(other * d, tp * d) for d in (1, -1, 2)}
    zpeer = [{"ep": ((z + i) % Z) * PLANE + me % PLANE, "tp": tp} for i in range(Z)]
    partner = {"ep": me, "tp": other}

    own = pl.ds(pl.multiple_of(tp * H, H), H)
    oth = pl.ds(pl.multiple_of(other * H, H), H)

    sent, groups = [], []

    class Group:
        def __init__(self, whole, out=None):
            self.whole = whole
            self.k = groups.append(self) or len(groups) - 1
            self.out = sent.append(self) or len(sent) - 1 if out is None else out.out

        def copy(self, src, dst, dev):
            self.dev = dev
            return pltpu.make_async_remote_copy(
                src_ref=src,
                dst_ref=dst,
                send_sem=ssem.at[self.out],
                recv_sem=rsem.at[self.k],
                device_id=dev,
                device_id_type=MESH,
            )

        def add(self, src, dst, dev):
            self.copy(src, dst, dev).start()

        def wait_recv(self):
            self.copy(self.whole, self.whole, self.dev).wait_recv()

        def wait_send(self):
            self.copy(self.whole, self.whole, self.dev).wait_send()

    class Sends:
        def __init__(self, whole, dev):
            self.whole, self.dev = whole, dev
            self.out = sent.append(self) or len(sent) - 1

        def wait_send(self):
            pltpu.make_async_remote_copy(
                src_ref=self.whole,
                dst_ref=self.whole,
                send_sem=ssem.at[self.out],
                recv_sem=rsem.at[0],
                device_id=self.dev,
                device_id_type=MESH,
            ).wait_send()

    def remote(src, dst, dev):
        group = Group(dst)
        group.add(src, dst, dev)
        return group

    local = {}

    def load(name, src, dst):
        copy = pltpu.make_async_copy(src, dst, lsem.at[len(local)])
        copy.start()
        local[name] = copy

    HOPS = ((2, 3), (1, 1), (-1, 2))
    BACK = ((2, 3), (-1, 1), (1, 2))

    class Gather:
        def __init__(self, buf):
            self.at = buf.at

        def spread(self, *todo):
            for d, b in HOPS:
                for a in todo:
                    self.across.add(self.at[a], self.at[SIDE * b + a], second[d])

        def start(self):
            at = self.at
            out = Sends(at[pl.ds(1, PLANE - 1)], partner)
            self.near, self.far = Group(at[pl.ds(1, 2)], out), Group(at[3], out)
            self.across = Group(at[pl.ds(SIDE, 3 * SIDE)], out)
            self.far.add(at[0], at[3], first[2])
            self.near.add(at[0], at[1], first[1])
            self.near.add(at[0], at[2], first[-1])

        def go(self):
            self.near.wait_recv()
            self.spread(1, 2)
            self.far.wait_recv()
            self.spread(3)

    class Ring:
        def __init__(self, buf):
            self.at, self.step = buf.at, 0
            self.out = Sends(buf.at[pl.ds(1, Z - 1)], partner)

        def start(self):
            at, t = self.at, self.step
            if t:
                self.group.wait_recv()
            up, down = max(0, 2 * t), max(0, 2 * t - 1)
            if t < 3:
                self.group = Group(at[pl.ds(2 * t + 1, 2)], self.out)
                self.group.add(at[up], at[2 * t + 2], zpeer[1])
                self.group.add(at[down], at[2 * t + 1], zpeer[-1])
            elif t == 3:
                self.group = Group(at[7], self.out)
                self.group.add(at[up, pl.ds(0, 2)], at[7, pl.ds(0, 2)], zpeer[1])
                self.group.add(at[down, pl.ds(2, 1)], at[7, pl.ds(2, 1)], zpeer[-1])
            self.step = t + 1

    small = (
        (tokens_h, tokens),
        (norm_mix_h, norm_mix),
        (routes_h, routes),
        (route_w_h, route_w),
        (norm_ffn_h, norm_ffn),
        (gate_vec_h, gate_vec),
    )
    barrier = pltpu.get_barrier_semaphore()
    greeted = [partner, first[1], first[-1], second[1], second[-1], zpeer[1], zpeer[-1]]
    load("s0", tokens_h, tokens)
    for dev in greeted:
        pl.semaphore_signal(barrier, inc=1, device_id=dev, device_id_type=MESH)

    for t, (src, dst) in enumerate(small):
        if t:
            load(f"s{t}", src, dst)
    for t, src in enumerate((dense_gate, dense_up, dense_down)):
        load(f"d{t}", src, wbuf.at[0, t])
    for t, (src, dst) in enumerate(((w_query, wq), (w_key, wk), (w_value, wv))):
        load(f"p{t}", src, dst)
    load("st", state, st)
    load("wo", w_out, wo_o)
    load("eg", exp_gate.at[:, own], we.at[tp, 0])
    load("eu", exp_up.at[:, own], we.at[tp, 1])
    load("ed", exp_down.at[0, :, own], we.at[tp, 2])

    local["s0"].wait()
    pl.semaphore_wait(barrier, len(greeted))

    def tell(k, *devs):
        for dev in devs:
            pl.semaphore_signal(gsem.at[k], inc=1, device_id=dev, device_id_type=MESH)

    tell(0, first[-1])
    tell(1, second[-1])
    tell(2, zpeer[1], zpeer[-1])

    c_tok = remote(tokens, tok_p, partner)
    weights = Ring(wbuf)
    for t in range(3):
        local[f"d{t}"].wait()
    weights.start()
    c_wo = Group(wo_p)
    c_wo.add(w_out.at[:, oth], wo_p.at[0], partner)
    c_wo.add(w_out.at[:, own], wo_p.at[1], partner)
    c_we = Group(we.at[tp])
    for t, src in enumerate((exp_gate.at[:, oth], exp_up.at[:, oth], exp_down.at[0, :, oth])):
        c_we.add(src, we.at[tp, t], partner)

    for t in (2, 3):
        local[f"s{t}"].wait()
    row_id = iota((EXPERTS, R), 0)
    wt = jnp.zeros((EXPERTS, R), F32)
    member = jnp.zeros((EXPERTS, R), F32)
    named = routes[...]
    gains = route_w[...].astype(F32)
    for t in range(routes.shape[0]):
        hit = row_id == named[t : t + 1, :]
        wt = wt + jnp.where(hit, gains[t : t + 1, :], 0.0)
        member = member + jnp.where(hit, 1.0, 0.0)
    blank = jnp.zeros((EXPERTS, 128 - R), F32)
    wt = jnp.concatenate([wt, blank], axis=1)
    member = jnp.concatenate([member, blank], axis=1)
    before = jnp.where(iota((128, 128), 0) < iota((128, 128), 1), 1.0, 0.0).astype(BF16)
    rank = dot(member.astype(BF16), before)
    slot_id = iota((SLOT, 128), 0).astype(F32)
    picks = []
    for e in range(EXPERTS):
        pick = jnp.where(rank[e : e + 1] == slot_id, member[e : e + 1], 0.0)
        picks.append(pick)
        scl_m[e] = pick * wt[e : e + 1]
    sel_m[...] = jnp.concatenate(picks, axis=0)
    for t in (1, 4, 5):
        local[f"s{t}"].wait()

    tok_f = tokens[...].astype(F32)
    c_tok.wait_recv()
    tok_pf = tok_p[...].astype(F32)
    total = jnp.sum(tok_f * tok_f, axis=1, keepdims=True) + jnp.sum(
        tok_pf * tok_pf, axis=1, keepdims=True
    )
    scale = lax.rsqrt(total / D + epsilon)
    gain_o = norm_mix[:, own]
    gain_p = norm_mix[:, oth]
    nx_o = (tok_f * scale * gain_o).astype(BF16)
    nx_p = (tok_pf * scale * gain_p).astype(BF16)

    def project(w):
        return (dot(nx_o, w[own, :]) + dot(nx_p, w[oth, :])).astype(BF16).astype(F32)

    local["p0"].wait()
    q = project(wq)
    pad = jnp.zeros((128 - R, HW), F32)
    q_t = jnp.concatenate([q, pad], axis=0).T
    pl.semaphore_wait(gsem.at[2], 2)
    tell(3, zpeer[2], zpeer[-2])
    for t in (1, 2):
        local[f"p{t}"].wait()
    local["st"].wait()
    k = project(wk) * hs ** (-0.5)
    v = project(wv)
    k_t = jnp.concatenate([k, pad], axis=0).T
    head_id = tp * heads
    decays = []
    for h in range(heads):
        cols = slice(h * hs, (h + 1) * hs)
        idv = jnp.zeros((1, 128), F32) + (head_id + h).astype(F32)
        decay = 1.0 - jnp.exp2(-3.0 - 2.0 * idv)
        decays.append(decay)
        rows = []
        for s in range(R):
            rows.append(jnp.sum(st[s, h] * q_t[cols, s : s + 1], axis=0, keepdims=True))
        qs = jnp.concatenate(rows, axis=0)
        qk = jnp.sum(q[:, cols] * k[:, cols], axis=1, keepdims=True)
        read = decay * qs + qk * v[:, cols]
        centre = jnp.mean(read, axis=1, keepdims=True)
        dev = read - centre
        spread = jnp.mean(dev * dev, axis=1, keepdims=True)
        ho_o[:, cols] = (dev * lax.rsqrt(spread + epsilon)).astype(BF16)
    c_ho = remote(ho_o, ho_p, partner)
    ho = ho_o[...]
    local["wo"].wait()
    a_o = dot(ho, wo_o[:, own]).astype(BF16).astype(F32)
    a_p = dot(ho, wo_o[:, oth]).astype(BF16).astype(F32)
    c_wo.wait_recv()
    c_ho.wait_recv()
    hp = ho_p[...]
    a_o = a_o + dot(hp, wo_p[0]).astype(BF16).astype(F32)
    a_p = a_p + dot(hp, wo_p[1]).astype(BF16).astype(F32)
    after = (tok_f + a_o).astype(BF16).astype(F32)
    after_p = (tok_pf + a_p).astype(BF16).astype(F32)
    squares = jnp.sum(after * after, axis=1, keepdims=True) + jnp.sum(
        after_p * after_p, axis=1, keepdims=True
    )
    normed = (after * lax.rsqrt(squares / D + epsilon) * norm_ffn[...]).astype(BF16)

    pl.semaphore_wait(gsem.at[0], 1)
    pl.semaphore_wait(gsem.at[1], 1)
    pl.semaphore_wait(gsem.at[3], 2)
    chosen = dot(sel_m[:, :R].astype(BF16), normed).astype(BF16)
    xs[...] = chosen.astype(F32).reshape(EXPERTS, SLOT, H).astype(BF16)
    xe_d[0] = normed
    seat = {i: j for j, i in enumerate(NEAR)}
    z_out = Sends(zr.at[pl.ds(1, Z - 1)], partner)
    z_near, z_far = Group(zr.at[pl.ds(1, 4)], z_out), Group(zr.at[pl.ds(5, 3)], z_out)
    for i in (2, 6, 1, 7, 4, 3, 5):
        group = z_near if i in NEAR[:5] else z_far
        group.add(xs.at[(z + i) % Z], zr.at[seat[Z - i]], zpeer[i])
    xe = (xe_a, xe_b, xe_c, xe_d)
    chunks = [Gather(buf) for buf in xe]
    chunks[DENSE].start()
    chunks[DENSE].spread(0)
    gate_row = gate_vec[...].astype(F32)
    gate_row = jnp.concatenate([gate_row[r : r + 1] for r in range(H // 128)], axis=1)
    logit = jnp.sum(normed.astype(F32) * gate_row, axis=1, keepdims=True)
    lg_s[...] = logit + jnp.zeros((R, 128), F32)
    c_lg = remote(lg_s, lg_r, partner)
    def new_state(h):
        cols = slice(h * hs, (h + 1) * hs)
        for s in range(R):
            ns[s, h] = decays[h] * st[s, h] + k_t[cols, s : s + 1] * v[s : s + 1, cols]

    new_state(0)

    for name in ("eg", "eu", "ed"):
        local[name].wait()
    c_we.wait_recv()
    for t in range(2):
        for n, dst in enumerate((w1.at[0, t], w1.at[1, t], w2.at[t])):
            dst[:FE] = we[t, n]
            dst[FE:] = jnp.zeros((128 - FE, H), BF16)
    new_state(1)
    comb = [scl_m[(z + i) % Z] for i in NEAR]
    comb.append(jnp.zeros((128 - EXPERTS * SLOT, 128), F32))
    comb = jnp.concatenate(comb, axis=0).T[:R, : EXPERTS * SLOT].astype(BF16)

    pe_o = (pe_o_a, pe_o_b, pe_o_c, pe_o_d)
    pe_s = (pe_s_a, pe_s_b, pe_s_c, pe_s_d)
    pe_r = (pe_r_a, pe_r_b, pe_r_c, pe_r_d)
    y32, yb = (y_a, y_b, y_c, y_d), (yb_a, yb_b, yb_c, yb_d)
    rb, sb = (rb_a, rb_b, rb_c, rb_d), (sb_a, sb_b, sb_c, sb_d)
    ra = (ra_a, ra_b, ra_c, ra_d)
    enter = (w1, w1, w1, w1d)
    leave = (w2, w2, w2, w2d)

    def matches(shape, row_dim, order, trips):
        row, slot = iota(shape, row_dim), iota(shape, 1 - row_dim)
        found, first_row = jnp.zeros(shape, F32), 0
        for i, first_slot, count in trips:
            if i in order:
                shift = SLOT * order.index(i) + first_slot - first_row
                hit = (slot - row == shift) & (row >= first_row) & (row < first_row + count)
                found = found + jnp.where(hit, 1.0, 0.0)
            first_row += count
        return found.astype(BF16)

    def pack(c):
        order = [i for i, _, _ in TRIPS[c]]
        parts = [(zr[seat[i]] if i else xs[z]).astype(F32) for i in order]
        if len(parts) % 2:
            parts.append(jnp.zeros((SLOT, H), F32))
        rows = jnp.concatenate(parts, axis=0).astype(BF16)
        take = matches((CHUNKS[c], SLOT * len(parts)), 0, order, TRIPS[c])
        xe[c][0] = dot(take, rows).astype(BF16)
        chunks[c].start()

    z_near.wait_recv()
    pack(0)
    pack(2)
    chunks[0].spread(0)
    chunks[2].spread(0)
    weights.start()
    chunks[DENSE].go()
    z_far.wait_recv()
    pack(1)
    chunks[1].spread(0)
    chunks[0].go()
    chunks[2].go()
    weights.start()
    chunks[1].go()

    c_pe, c_rb, c_ra = {}, {}, {}

    def before_act(c):
        n = CHUNKS[c]
        chunks[c].across.wait_recv()
        pre = dot_t(xe[c][...].reshape(PLANE * n, H), enter[c][...].reshape(512, H))
        pe_o[c][...] = pre
        for b in range(SIDE):
            for a in range(SIDE):
                f = SIDE * b + a
                pe_s[c][SIDE * a + b] = pre[f * n : (f + 1) * n].astype(BF16)
        c_pe[c] = remote(pe_s[c], pe_r[c], partner)

    def act(c):
        n = CHUNKS[c]
        c_pe[c].wait_recv()
        pre = pe_o[c][...] + pe_r[c][...].astype(F32).reshape(PLANE * n, 512)
        hidden = (silu(pre[:, :256]) * pre[:, 256:]).astype(BF16)
        down = leave[c][...].reshape(256, H)
        gone = dot(hidden[SIDE * n :], down)
        yb[c][...] = gone.reshape(3 * SIDE, n, H).astype(BF16)
        out, at = yb[c].at, rb[c].at
        c_rb[c] = Group(rb[c])
        for d, b in BACK:
            c_rb[c].add(out[pl.ds(SIDE * (b - 1), SIDE)], at[b - 1], second[d])
        y32[c][...] = dot(hidden[: SIDE * n], down).reshape(SIDE, n, H)

    def sum_second(c):
        c_rb[c].wait_recv()
        total = y32[c][...]
        for b in range(3):
            total = total + rb[c][b].astype(F32)
        sb[c][...] = total[1:].astype(BF16)
        c_ra[c] = Group(ra[c])
        for d, a in BACK:
            c_ra[c].add(sb[c].at[a - 1], ra[c].at[a - 1], first[d])
        y32[c][0] = total[0]

    c_ret = Group(zret.at[pl.ds(1, Z - 1)])

    def sum_first(c):
        c_ra[c].wait_recv()
        total = y32[c][0]
        for a in range(3):
            total = total + ra[c][a].astype(F32)
        return total

    def give_back(c, *order):
        tot[sum(CHUNKS[:c]) : sum(CHUNKS[: c + 1])] = sum_first(c)
        done = tot[: sum(CHUNKS[: c + 1])]
        pad = -done.shape[0] % 16
        if pad:
            done = jnp.concatenate([done, jnp.zeros((pad, H), F32)], axis=0)
        put = matches((SLOT * len(order), done.shape[0]), 1, order, sum(TRIPS[: c + 1], ()))
        rows = dot(put, done.astype(BF16))
        for n, i in enumerate(order):
            block = rows[n * SLOT : (n + 1) * SLOT].astype(BF16)
            if i == 0:
                zret[0] = block
            else:
                zs[i] = block
                c_ret.add(zs.at[i], zret.at[seat[Z - i]], zpeer[i])

    before_act(0)
    weights.start()
    act(0)
    before_act(1)
    before_act(2)
    act(1)
    weights.start()
    for j in range(Z):
        for t, dst in enumerate((w1d.at[0, j], w1d.at[1, j], w2d.at[j])):
            dst[:FD] = wbuf[j, t]
            dst[FD:] = jnp.zeros((32 - FD, H), BF16)
    before_act(DENSE)
    act(2)
    sum_second(0)
    act(DENSE)
    sum_second(1)
    give_back(0, 1, 2, 6)
    sum_second(2)
    give_back(1, 3, 4, 5)
    sum_second(DENSE)
    give_back(2, 7, 0)
    dense = sum_first(DENSE)

    c_lg.wait_recv()
    open_ = 1.0 / (1.0 + jnp.exp(-(lg_s[:, :1] + lg_r[:, :1])))
    c_ret.wait_recv()
    back = zret[...].astype(F32).reshape(EXPERTS * SLOT, H).astype(BF16)
    moe = dot(comb, back)
    mixed[...] = (after + moe + open_ * dense).astype(BF16)
    for group in sent:
        group.wait_send()
    assert (len(groups), len(sent), len(local)) == (GROUPS, SENDS, LOADS), (len(groups), len(sent))


def store(a_in, b_in, a_out, b_out, sems):
    first = pltpu.make_async_copy(b_in, b_out, sems.at[0])
    second = pltpu.make_async_copy(a_in, a_out, sems.at[1])
    first.start()
    second.start()
    first.wait()
    second.wait()


def body(
    tokens,
    state,
    norm_mix,
    w_query,
    w_key,
    w_value,
    w_out,
    norm_ffn,
    gate_vector,
    dense_gate,
    dense_up,
    dense_down,
    exp_gate,
    exp_up,
    exp_down,
    routes,
    route_w,
):
    R, H = tokens.shape
    heads, hs = state.shape[1], state.shape[2]
    HW = heads * hs
    FE = exp_gate.shape[2]
    FD = dense_gate.shape[1]
    Z = EXPERTS
    per_chunk = lambda make: [make(n) for n in CHUNKS]
    vm = pl.BlockSpec(memory_space=pltpu.VMEM)
    hbm = pl.BlockSpec(memory_space=pltpu.HBM)
    V = pltpu.VMEM
    sem = lambda *shape: pltpu.SemaphoreType.DMA(shape)
    operands = (
        tokens,
        norm_mix.reshape(1, -1),
        routes.T,
        route_w.T,
        norm_ffn.reshape(1, -1),
        gate_vector.reshape(-1, 128),
        state,
        w_query,
        w_key,
        w_value,
        w_out,
        dense_gate.T,
        dense_up.T,
        dense_down,
        exp_gate[0].T,
        exp_up[0].T,
        exp_down,
    )
    held = [pltpu.with_memory_space_constraint(x, pltpu.HBM) for x in operands]
    mixed, new_state = pl.pallas_call(
        kernel,
        out_shape=(pltpu.VMEM((R, H), BF16), pltpu.VMEM(state.shape, F32)),
        in_specs=[hbm] * 17,
        out_specs=(vm, vm),
        scratch_shapes=[
            V((R, H), BF16),
            V((1, 2 * H), F32),
            V((routes.shape[1], R), jnp.int32),
            V((routes.shape[1], R), BF16),
            V((1, H), F32),
            V((H // 128, 128), BF16),
            V((R, H), BF16),
            V((2 * H, HW), BF16),
            V((2 * H, HW), BF16),
            V((2 * H, HW), BF16),
            V((HW, 2 * H), BF16),
            V((2, HW, H), BF16),
            V((2, 3, FE, H), BF16),
            V(state.shape, F32),
            V((R, HW), BF16),
            V((R, HW), BF16),
            V((EXPERTS * SLOT, 128), F32),
            V((EXPERTS, SLOT, 128), F32),
            V((R, 128), F32),
            V((R, 128), F32),
            V((Z, 3, FD, H), BF16),
            V((2, 2, 128, H), BF16),
            V((2, 128, H), BF16),
            V((2, Z, 32, H), BF16),
            V((Z, 32, H), BF16),
            V((EXPERTS, SLOT, H), BF16),
            V((Z, SLOT, H), BF16),
            *per_chunk(lambda n: V((PLANE, n, H), BF16)),
            *per_chunk(lambda n: V((PLANE * n, 512), F32)),
            *per_chunk(lambda n: V((PLANE, n, 512), BF16)),
            *per_chunk(lambda n: V((PLANE, n, 512), BF16)),
            *per_chunk(lambda n: V((SIDE, n, H), F32)),
            *per_chunk(lambda n: V((3 * SIDE, n, H), BF16)),
            *per_chunk(lambda n: V((3, SIDE, n, H), BF16)),
            *per_chunk(lambda n: V((3, n, H), BF16)),
            *per_chunk(lambda n: V((3, n, H), BF16)),
            V((sum(CHUNKS[:DENSE]), H), F32),
            V((Z, SLOT, H), BF16),
            V((Z, SLOT, H), BF16),
            sem(LOADS),
            sem(SENDS),
            sem(GROUPS),
            pltpu.SemaphoreType.REGULAR((4,)),
        ],
        compiler_params=pltpu.CompilerParams(
            collective_id=0, has_side_effects=True, vmem_limit_bytes=50 * 1024 * 1024
        ),
        name="layer",
    )(
        *held
    )
    return pl.pallas_call(
        store,
        out_shape=(
            jax.ShapeDtypeStruct((R, H), BF16),
            jax.ShapeDtypeStruct(state.shape, F32),
        ),
        in_specs=[vm, vm],
        out_specs=(hbm, hbm),
        scratch_shapes=[sem(2)],
        name="store",
    )(
        pltpu.with_memory_space_constraint(mixed, pltpu.VMEM),
        pltpu.with_memory_space_constraint(new_state, pltpu.VMEM),
    )


def solution(mesh):
    return jax.shard_map(
        body,
        mesh=mesh,
        in_specs=(
            P("ep", "tp"),
            P("ep", "tp", None, None),
            P(),
            P(None, "tp"),
            P(None, "tp"),
            P(None, "tp"),
            P("tp", None),
            P("tp"),
            P("tp"),
            P("tp", "ep"),
            P("tp", "ep"),
            P("ep", "tp"),
            P("ep", None, "tp"),
            P("ep", None, "tp"),
            P("ep", "tp", None),
            P("ep", None),
            P("ep", None),
        ),
        out_specs=(P("ep", "tp"), P("ep", "tp", None, None)),
        check_vma=False,
    )
```

```python
import functools

import jax
import jax.numpy as jnp
from jax import lax
from jax.experimental import pallas as pl
from jax.experimental.pallas import tpu as pltpu
from jax.sharding import PartitionSpec as P

EXPERTS = 8
CAP = 5
SLOT = 8
SIDE = 4
PLANE = SIDE * SIDE
NEAR = (0, 1, 7, 2, 6, 3, 5, 4)
TRIPS = (
    ((1, 0, CAP), (2, 0, CAP), (6, 0, CAP), (7, 0, 1)),
    ((3, 0, CAP), (4, 0, CAP), (5, 0, CAP), (7, 1, 1)),
    ((7, 2, CAP - 2), (0, 0, CAP)),
)
CHUNKS = (16, 16, 8, 16)
DENSE = len(CHUNKS) - 1
GROUPS = 36
SENDS = 24
LOADS = 17
epsilon = 1e-06
MESH = pl.DeviceIdType.MESH
F32 = jnp.float32
BF16 = jnp.bfloat16


def dot(a, b):
    return jnp.dot(a, b, preferred_element_type=F32)


def dot_t(a, b):
    return lax.dot_general(a, b, (((1,), (1,)), ((), ())), preferred_element_type=F32)


def silu(v):
    return v / (1.0 + jnp.exp(-v))


def iota(shape, dim):
    return lax.broadcasted_iota(jnp.int32, shape, dim)


def kernel(
    tokens_h,
    norm_mix_h,
    routes_h,
    route_w_h,
    norm_ffn_h,
    gate_vec_h,
    state,
    w_query,
    w_key,
    w_value,
    w_out,
    dense_gate,
    dense_up,
    dense_down,
    exp_gate,
    exp_up,
    exp_down,
    mixed,
    ns,
    tokens,
    norm_mix,
    routes,
    route_w,
    norm_ffn,
    gate_vec,
    tok_p,
    wq,
    wk,
    wv,
    wo_o,
    wo_p,
    we,
    st,
    ho_o,
    ho_p,
    sel_m,
    scl_m,
    lg_s,
    lg_r,
    wbuf,
    w1,
    w2,
    w1d,
    w2d,
    xs,
    zr,
    xe_a,
    xe_b,
    xe_c,
    xe_d,
    pe_o_a,
    pe_o_b,
    pe_o_c,
    pe_o_d,
    pe_s_a,
    pe_s_b,
    pe_s_c,
    pe_s_d,
    pe_r_a,
    pe_r_b,
    pe_r_c,
    pe_r_d,
    y_a,
    y_b,
    y_c,
    y_d,
    yb_a,
    yb_b,
    yb_c,
    yb_d,
    rb_a,
    rb_b,
    rb_c,
    rb_d,
    sb_a,
    sb_b,
    sb_c,
    sb_d,
    ra_a,
    ra_b,
    ra_c,
    ra_d,
    tot,
    zs,
    zret,
    lsem,
    ssem,
    rsem,
    gsem,
):
    R, H = tokens.shape
    D = 2 * H
    heads, hs = state.shape[1], state.shape[2]
    HW = heads * hs
    FE = we.shape[2]
    FD = wbuf.shape[2]
    Z = EXPERTS
    me = lax.axis_index("ep")
    tp = lax.axis_index("tp")
    other = 1 - tp
    z, y_at, x_at = me // PLANE, (me // SIDE) % SIDE, me % SIDE

    def in_plane(dy, dx):
        return {
            "ep": z * PLANE + ((y_at + dy + SIDE) % SIDE) * SIDE + (x_at + dx + SIDE) % SIDE,
            "tp": tp,
        }

    first = {d: in_plane(tp * d, other * d) for d in (1, -1, 2)}
    second = {d: in_plane(other * d, tp * d) for d in (1, -1, 2)}
    zpeer = [{"ep": ((z + i) % Z) * PLANE + me % PLANE, "tp": tp} for i in range(Z)]
    partner = {"ep": me, "tp": other}

    own = pl.ds(pl.multiple_of(tp * H, H), H)
    oth = pl.ds(pl.multiple_of(other * H, H), H)

    sent, groups = [], []

    class Group:
        def __init__(self, whole, out=None):
            self.whole = whole
            self.k = groups.append(self) or len(groups) - 1
            self.out = sent.append(self) or len(sent) - 1 if out is None else out.out

        def copy(self, src, dst, dev):
            self.dev = dev
            return pltpu.make_async_remote_copy(
                src_ref=src,
                dst_ref=dst,
                send_sem=ssem.at[self.out],
                recv_sem=rsem.at[self.k],
                device_id=dev,
                device_id_type=MESH,
            )

        def add(self, src, dst, dev):
            self.copy(src, dst, dev).start()

        def wait_recv(self):
            self.copy(self.whole, self.whole, self.dev).wait_recv()

        def wait_send(self):
            self.copy(self.whole, self.whole, self.dev).wait_send()

    class Sends:
        def __init__(self, whole, dev):
            self.whole, self.dev = whole, dev
            self.out = sent.append(self) or len(sent) - 1

        def wait_send(self):
            pltpu.make_async_remote_copy(
                src_ref=self.whole,
                dst_ref=self.whole,
                send_sem=ssem.at[self.out],
                recv_sem=rsem.at[0],
                device_id=self.dev,
                device_id_type=MESH,
            ).wait_send()

    def remote(src, dst, dev):
        group = Group(dst)
        group.add(src, dst, dev)
        return group

    local = {}

    def load(name, src, dst):
        copy = pltpu.make_async_copy(src, dst, lsem.at[len(local)])
        copy.start()
        local[name] = copy

    HOPS = ((2, 3), (1, 1), (-1, 2))
    BACK = ((2, 3), (-1, 1), (1, 2))

    class Gather:
        def __init__(self, buf):
            self.at = buf.at

        def spread(self, *todo):
            for d, b in HOPS:
                for a in todo:
                    self.across.add(self.at[a], self.at[SIDE * b + a], second[d])

        def start(self):
            at = self.at
            out = Sends(at[pl.ds(1, PLANE - 1)], partner)
            self.near, self.far = Group(at[pl.ds(1, 2)], out), Group(at[3], out)
            self.across = Group(at[pl.ds(SIDE, 3 * SIDE)], out)
            self.far.add(at[0], at[3], first[2])
            self.near.add(at[0], at[1], first[1])
            self.near.add(at[0], at[2], first[-1])

        def go(self):
            self.near.wait_recv()
            self.spread(1, 2)
            self.far.wait_recv()
            self.spread(3)

    class Ring:
        def __init__(self, buf):
            self.at, self.step = buf.at, 0
            self.out = Sends(buf.at[pl.ds(1, Z - 1)], partner)

        def start(self):
            at, t = self.at, self.step
            if t:
                self.group.wait_recv()
            up, down = max(0, 2 * t), max(0, 2 * t - 1)
            if t < 3:
                self.group = Group(at[pl.ds(2 * t + 1, 2)], self.out)
                self.group.add(at[up], at[2 * t + 2], zpeer[1])
                self.group.add(at[down], at[2 * t + 1], zpeer[-1])
            elif t == 3:
                self.group = Group(at[7], self.out)
                self.group.add(at[up, pl.ds(0, 2)], at[7, pl.ds(0, 2)], zpeer[1])
                self.group.add(at[down, pl.ds(2, 1)], at[7, pl.ds(2, 1)], zpeer[-1])
            self.step = t + 1

    small = (
        (tokens_h, tokens),
        (norm_mix_h, norm_mix),
        (routes_h, routes),
        (route_w_h, route_w),
        (norm_ffn_h, norm_ffn),
        (gate_vec_h, gate_vec),
    )
    barrier = pltpu.get_barrier_semaphore()
    greeted = [partner, first[1], first[-1], second[1], second[-1], zpeer[1], zpeer[-1]]
    load("s0", tokens_h, tokens)
    for dev in greeted:
        pl.semaphore_signal(barrier, inc=1, device_id=dev, device_id_type=MESH)

    for t, (src, dst) in enumerate(small):
        if t:
            load(f"s{t}", src, dst)
    for t, src in enumerate((dense_gate, dense_up, dense_down)):
        load(f"d{t}", src, wbuf.at[0, t])
    for t, (src, dst) in enumerate(((w_query, wq), (w_key, wk), (w_value, wv))):
        load(f"p{t}", src, dst)
    load("st", state, st)
    load("wo", w_out, wo_o)
    load("eg", exp_gate.at[:, own], we.at[tp, 0])
    load("eu", exp_up.at[:, own], we.at[tp, 1])
    load("ed", exp_down.at[0, :, own], we.at[tp, 2])

    local["s0"].wait()
    pl.semaphore_wait(barrier, len(greeted))

    def tell(k, *devs):
        for dev in devs:
            pl.semaphore_signal(gsem.at[k], inc=1, device_id=dev, device_id_type=MESH)

    tell(0, first[-1])
    tell(1, second[-1])
    tell(2, zpeer[1], zpeer[-1])

    c_tok = remote(tokens, tok_p, partner)
    weights = Ring(wbuf)
    for t in range(3):
        local[f"d{t}"].wait()
    weights.start()
    c_wo = Group(wo_p)
    c_wo.add(w_out.at[:, oth], wo_p.at[0], partner)
    c_wo.add(w_out.at[:, own], wo_p.at[1], partner)
    c_we = Group(we.at[tp])
    for t, src in enumerate((exp_gate.at[:, oth], exp_up.at[:, oth], exp_down.at[0, :, oth])):
        c_we.add(src, we.at[tp, t], partner)

    for t in (2, 3):
        local[f"s{t}"].wait()
    row_id = iota((EXPERTS, R), 0)
    wt = jnp.zeros((EXPERTS, R), F32)
    member = jnp.zeros((EXPERTS, R), F32)
    named = routes[...]
    gains = route_w[...].astype(F32)
    for t in range(routes.shape[0]):
        hit = row_id == named[t : t + 1, :]
        wt = wt + jnp.where(hit, gains[t : t + 1, :], 0.0)
        member = member + jnp.where(hit, 1.0, 0.0)
    blank = jnp.zeros((EXPERTS, 128 - R), F32)
    wt = jnp.concatenate([wt, blank], axis=1)
    member = jnp.concatenate([member, blank], axis=1)
    before = jnp.where(iota((128, 128), 0) < iota((128, 128), 1), 1.0, 0.0).astype(BF16)
    rank = dot(member.astype(BF16), before)
    slot_id = iota((SLOT, 128), 0).astype(F32)
    picks = []
    for e in range(EXPERTS):
        pick = jnp.where(rank[e : e + 1] == slot_id, member[e : e + 1], 0.0)
        picks.append(pick)
        scl_m[e] = pick * wt[e : e + 1]
    sel_m[...] = jnp.concatenate(picks, axis=0)
    for t in (1, 4, 5):
        local[f"s{t}"].wait()

    tok_f = tokens[...].astype(F32)
    c_tok.wait_recv()
    tok_pf = tok_p[...].astype(F32)
    total = jnp.sum(tok_f * tok_f, axis=1, keepdims=True) + jnp.sum(
        tok_pf * tok_pf, axis=1, keepdims=True
    )
    scale = lax.rsqrt(total / D + epsilon)
    gain_o = norm_mix[:, own]
    gain_p = norm_mix[:, oth]
    nx_o = (tok_f * scale * gain_o).astype(BF16)
    nx_p = (tok_pf * scale * gain_p).astype(BF16)

    def project(w):
        return (dot(nx_o, w[own, :]) + dot(nx_p, w[oth, :])).astype(BF16).astype(F32)

    local["p0"].wait()
    q = project(wq)
    pad = jnp.zeros((128 - R, HW), F32)
    q_t = jnp.concatenate([q, pad], axis=0).T
    pl.semaphore_wait(gsem.at[2], 2)
    tell(3, zpeer[2], zpeer[-2])
    for t in (1, 2):
        local[f"p{t}"].wait()
    local["st"].wait()
    k = project(wk) * hs ** (-0.5)
    v = project(wv)
    k_t = jnp.concatenate([k, pad], axis=0).T
    head_id = tp * heads
    decays = []
    for h in range(heads):
        cols = slice(h * hs, (h + 1) * hs)
        idv = jnp.zeros((1, 128), F32) + (head_id + h).astype(F32)
        decay = 1.0 - jnp.exp2(-3.0 - 2.0 * idv)
        decays.append(decay)
        rows = []
        for s in range(R):
            rows.append(jnp.sum(st[s, h] * q_t[cols, s : s + 1], axis=0, keepdims=True))
        qs = jnp.concatenate(rows, axis=0)
        qk = jnp.sum(q[:, cols] * k[:, cols], axis=1, keepdims=True)
        read = decay * qs + qk * v[:, cols]
        centre = jnp.mean(read, axis=1, keepdims=True)
        dev = read - centre
        spread = jnp.mean(dev * dev, axis=1, keepdims=True)
        ho_o[:, cols] = (dev * lax.rsqrt(spread + epsilon)).astype(BF16)
    c_ho = remote(ho_o, ho_p, partner)
    ho = ho_o[...]
    local["wo"].wait()
    a_o = dot(ho, wo_o[:, own]).astype(BF16).astype(F32)
    a_p = dot(ho, wo_o[:, oth]).astype(BF16).astype(F32)
    c_wo.wait_recv()
    c_ho.wait_recv()
    hp = ho_p[...]
    a_o = a_o + dot(hp, wo_p[0]).astype(BF16).astype(F32)
    a_p = a_p + dot(hp, wo_p[1]).astype(BF16).astype(F32)
    after = (tok_f + a_o).astype(BF16).astype(F32)
    after_p = (tok_pf + a_p).astype(BF16).astype(F32)
    squares = jnp.sum(after * after, axis=1, keepdims=True) + jnp.sum(
        after_p * after_p, axis=1, keepdims=True
    )
    normed = (after * lax.rsqrt(squares / D + epsilon) * norm_ffn[...]).astype(BF16)

    pl.semaphore_wait(gsem.at[0], 1)
    pl.semaphore_wait(gsem.at[1], 1)
    pl.semaphore_wait(gsem.at[3], 2)
    chosen = dot(sel_m[:, :R].astype(BF16), normed).astype(BF16)
    xs[...] = chosen.astype(F32).reshape(EXPERTS, SLOT, H).astype(BF16)
    xe_d[0] = normed
    seat = {i: j for j, i in enumerate(NEAR)}
    z_out = Sends(zr.at[pl.ds(1, Z - 1)], partner)
    z_near, z_far = Group(zr.at[pl.ds(1, 4)], z_out), Group(zr.at[pl.ds(5, 3)], z_out)
    for i in (2, 6, 1, 7, 4, 3, 5):
        group = z_near if i in NEAR[:5] else z_far
        group.add(xs.at[(z + i) % Z], zr.at[seat[Z - i]], zpeer[i])
    xe = (xe_a, xe_b, xe_c, xe_d)
    chunks = [Gather(buf) for buf in xe]
    chunks[DENSE].start()
    chunks[DENSE].spread(0)
    gate_row = gate_vec[...].astype(F32)
    gate_row = jnp.concatenate([gate_row[r : r + 1] for r in range(H // 128)], axis=1)
    logit = jnp.sum(normed.astype(F32) * gate_row, axis=1, keepdims=True)
    lg_s[...] = logit + jnp.zeros((R, 128), F32)
    c_lg = remote(lg_s, lg_r, partner)
    def new_state(h):
        cols = slice(h * hs, (h + 1) * hs)
        for s in range(R):
            ns[s, h] = decays[h] * st[s, h] + k_t[cols, s : s + 1] * v[s : s + 1, cols]

    new_state(0)

    for name in ("eg", "eu", "ed"):
        local[name].wait()
    c_we.wait_recv()
    for t in range(2):
        for n, dst in enumerate((w1.at[0, t], w1.at[1, t], w2.at[t])):
            dst[:FE] = we[t, n]
            dst[FE:] = jnp.zeros((128 - FE, H), BF16)
    new_state(1)
    comb = [scl_m[(z + i) % Z] for i in NEAR]
    comb.append(jnp.zeros((128 - EXPERTS * SLOT, 128), F32))
    comb = jnp.concatenate(comb, axis=0).T[:R, : EXPERTS * SLOT].astype(BF16)

    pe_o = (pe_o_a, pe_o_b, pe_o_c, pe_o_d)
    pe_s = (pe_s_a, pe_s_b, pe_s_c, pe_s_d)
    pe_r = (pe_r_a, pe_r_b, pe_r_c, pe_r_d)
    y32, yb = (y_a, y_b, y_c, y_d), (yb_a, yb_b, yb_c, yb_d)
    rb, sb = (rb_a, rb_b, rb_c, rb_d), (sb_a, sb_b, sb_c, sb_d)
    ra = (ra_a, ra_b, ra_c, ra_d)
    enter = (w1, w1, w1, w1d)
    leave = (w2, w2, w2, w2d)

    def matches(shape, row_dim, order, trips):
        row, slot = iota(shape, row_dim), iota(shape, 1 - row_dim)
        found, first_row = jnp.zeros(shape, F32), 0
        for i, first_slot, count in trips:
            if i in order:
                shift = SLOT * order.index(i) + first_slot - first_row
                hit = (slot - row == shift) & (row >= first_row) & (row < first_row + count)
                found = found + jnp.where(hit, 1.0, 0.0)
            first_row += count
        return found.astype(BF16)

    def pack(c):
        order = [i for i, _, _ in TRIPS[c]]
        parts = [(zr[seat[i]] if i else xs[z]).astype(F32) for i in order]
        if len(parts) % 2:
            parts.append(jnp.zeros((SLOT, H), F32))
        rows = jnp.concatenate(parts, axis=0).astype(BF16)
        take = matches((CHUNKS[c], SLOT * len(parts)), 0, order, TRIPS[c])
        xe[c][0] = dot(take, rows).astype(BF16)
        chunks[c].start()

    z_near.wait_recv()
    pack(0)
    pack(2)
    chunks[0].spread(0)
    chunks[2].spread(0)
    weights.start()
    z_far.wait_recv()
    pack(1)
    chunks[1].spread(0)
    chunks[0].go()
    chunks[2].go()
    weights.start()
    chunks[1].go()
    chunks[DENSE].go()

    c_pe, c_rb, c_ra = {}, {}, {}

    def before_act(c):
        n = CHUNKS[c]
        chunks[c].across.wait_recv()
        pre = dot_t(xe[c][...].reshape(PLANE * n, H), enter[c][...].reshape(512, H))
        pe_o[c][...] = pre
        for b in range(SIDE):
            for a in range(SIDE):
                f = SIDE * b + a
                pe_s[c][SIDE * a + b] = pre[f * n : (f + 1) * n].astype(BF16)
        c_pe[c] = remote(pe_s[c], pe_r[c], partner)

    def act(c):
        n = CHUNKS[c]
        c_pe[c].wait_recv()
        pre = pe_o[c][...] + pe_r[c][...].astype(F32).reshape(PLANE * n, 512)
        hidden = (silu(pre[:, :256]) * pre[:, 256:]).astype(BF16)
        down = leave[c][...].reshape(256, H)
        gone = dot(hidden[SIDE * n :], down)
        yb[c][...] = gone.reshape(3 * SIDE, n, H).astype(BF16)
        out, at = yb[c].at, rb[c].at
        c_rb[c] = Group(rb[c])
        for d, b in BACK:
            c_rb[c].add(out[pl.ds(SIDE * (b - 1), SIDE)], at[b - 1], second[d])
        y32[c][...] = dot(hidden[: SIDE * n], down).reshape(SIDE, n, H)

    def sum_second(c):
        c_rb[c].wait_recv()
        total = y32[c][...]
        for b in range(3):
            total = total + rb[c][b].astype(F32)
        sb[c][...] = total[1:].astype(BF16)
        c_ra[c] = Group(ra[c])
        for d, a in BACK:
            c_ra[c].add(sb[c].at[a - 1], ra[c].at[a - 1], first[d])
        y32[c][0] = total[0]

    c_ret = Group(zret.at[pl.ds(1, Z - 1)])

    def sum_first(c):
        c_ra[c].wait_recv()
        total = y32[c][0]
        for a in range(3):
            total = total + ra[c][a].astype(F32)
        return total

    def give_back(c, *order):
        tot[sum(CHUNKS[:c]) : sum(CHUNKS[: c + 1])] = sum_first(c)
        done = tot[: sum(CHUNKS[: c + 1])]
        pad = -done.shape[0] % 16
        if pad:
            done = jnp.concatenate([done, jnp.zeros((pad, H), F32)], axis=0)
        put = matches((SLOT * len(order), done.shape[0]), 1, order, sum(TRIPS[: c + 1], ()))
        rows = dot(put, done.astype(BF16))
        for n, i in enumerate(order):
            block = rows[n * SLOT : (n + 1) * SLOT].astype(BF16)
            if i == 0:
                zret[0] = block
            else:
                zs[i] = block
                c_ret.add(zs.at[i], zret.at[seat[Z - i]], zpeer[i])

    before_act(0)
    weights.start()
    act(0)
    before_act(1)
    before_act(2)
    act(1)
    weights.start()
    for j in range(Z):
        for t, dst in enumerate((w1d.at[0, j], w1d.at[1, j], w2d.at[j])):
            dst[:FD] = wbuf[j, t]
            dst[FD:] = jnp.zeros((32 - FD, H), BF16)
    before_act(DENSE)
    act(2)
    act(DENSE)
    sum_second(0)
    sum_second(1)
    give_back(0, 1, 2, 6)
    sum_second(2)
    give_back(1, 3, 4, 5)
    sum_second(DENSE)
    give_back(2, 7, 0)
    dense = sum_first(DENSE)

    c_lg.wait_recv()
    open_ = 1.0 / (1.0 + jnp.exp(-(lg_s[:, :1] + lg_r[:, :1])))
    c_ret.wait_recv()
    back = zret[...].astype(F32).reshape(EXPERTS * SLOT, H).astype(BF16)
    moe = dot(comb, back)
    mixed[...] = (after + moe + open_ * dense).astype(BF16)
    for group in sent:
        group.wait_send()
    assert (len(groups), len(sent), len(local)) == (GROUPS, SENDS, LOADS), (len(groups), len(sent))


def store(a_in, b_in, a_out, b_out, sems):
    first = pltpu.make_async_copy(b_in, b_out, sems.at[0])
    second = pltpu.make_async_copy(a_in, a_out, sems.at[1])
    first.start()
    second.start()
    first.wait()
    second.wait()


def body(
    tokens,
    state,
    norm_mix,
    w_query,
    w_key,
    w_value,
    w_out,
    norm_ffn,
    gate_vector,
    dense_gate,
    dense_up,
    dense_down,
    exp_gate,
    exp_up,
    exp_down,
    routes,
    route_w,
):
    R, H = tokens.shape
    heads, hs = state.shape[1], state.shape[2]
    HW = heads * hs
    FE = exp_gate.shape[2]
    FD = dense_gate.shape[1]
    Z = EXPERTS
    per_chunk = lambda make: [make(n) for n in CHUNKS]
    vm = pl.BlockSpec(memory_space=pltpu.VMEM)
    hbm = pl.BlockSpec(memory_space=pltpu.HBM)
    V = pltpu.VMEM
    sem = lambda *shape: pltpu.SemaphoreType.DMA(shape)
    operands = (
        tokens,
        norm_mix.reshape(1, -1),
        routes.T,
        route_w.T,
        norm_ffn.reshape(1, -1),
        gate_vector.reshape(-1, 128),
        state,
        w_query,
        w_key,
        w_value,
        w_out,
        dense_gate.T,
        dense_up.T,
        dense_down,
        exp_gate[0].T,
        exp_up[0].T,
        exp_down,
    )
    held = [pltpu.with_memory_space_constraint(x, pltpu.HBM) for x in operands]
    mixed, new_state = pl.pallas_call(
        kernel,
        out_shape=(pltpu.VMEM((R, H), BF16), pltpu.VMEM(state.shape, F32)),
        in_specs=[hbm] * 17,
        out_specs=(vm, vm),
        scratch_shapes=[
            V((R, H), BF16),
            V((1, 2 * H), F32),
            V((routes.shape[1], R), jnp.int32),
            V((routes.shape[1], R), BF16),
            V((1, H), F32),
            V((H // 128, 128), BF16),
            V((R, H), BF16),
            V((2 * H, HW), BF16),
            V((2 * H, HW), BF16),
            V((2 * H, HW), BF16),
            V((HW, 2 * H), BF16),
            V((2, HW, H), BF16),
            V((2, 3, FE, H), BF16),
            V(state.shape, F32),
            V((R, HW), BF16),
            V((R, HW), BF16),
            V((EXPERTS * SLOT, 128), F32),
            V((EXPERTS, SLOT, 128), F32),
            V((R, 128), F32),
            V((R, 128), F32),
            V((Z, 3, FD, H), BF16),
            V((2, 2, 128, H), BF16),
            V((2, 128, H), BF16),
            V((2, Z, 32, H), BF16),
            V((Z, 32, H), BF16),
            V((EXPERTS, SLOT, H), BF16),
            V((Z, SLOT, H), BF16),
            *per_chunk(lambda n: V((PLANE, n, H), BF16)),
            *per_chunk(lambda n: V((PLANE * n, 512), F32)),
            *per_chunk(lambda n: V((PLANE, n, 512), BF16)),
            *per_chunk(lambda n: V((PLANE, n, 512), BF16)),
            *per_chunk(lambda n: V((SIDE, n, H), F32)),
            *per_chunk(lambda n: V((3 * SIDE, n, H), BF16)),
            *per_chunk(lambda n: V((3, SIDE, n, H), BF16)),
            *per_chunk(lambda n: V((3, n, H), BF16)),
            *per_chunk(lambda n: V((3, n, H), BF16)),
            V((sum(CHUNKS[:DENSE]), H), F32),
            V((Z, SLOT, H), BF16),
            V((Z, SLOT, H), BF16),
            sem(LOADS),
            sem(SENDS),
            sem(GROUPS),
            pltpu.SemaphoreType.REGULAR((4,)),
        ],
        compiler_params=pltpu.CompilerParams(
            collective_id=0, has_side_effects=True, vmem_limit_bytes=50 * 1024 * 1024
        ),
        name="layer",
    )(
        *held
    )
    return pl.pallas_call(
        store,
        out_shape=(
            jax.ShapeDtypeStruct((R, H), BF16),
            jax.ShapeDtypeStruct(state.shape, F32),
        ),
        in_specs=[vm, vm],
        out_specs=(hbm, hbm),
        scratch_shapes=[sem(2)],
        name="store",
    )(
        pltpu.with_memory_space_constraint(mixed, pltpu.VMEM),
        pltpu.with_memory_space_constraint(new_state, pltpu.VMEM),
    )


def solution(mesh):
    return jax.shard_map(
        body,
        mesh=mesh,
        in_specs=(
            P("ep", "tp"),
            P("ep", "tp", None, None),
            P(),
            P(None, "tp"),
            P(None, "tp"),
            P(None, "tp"),
            P("tp", None),
            P("tp"),
            P("tp"),
            P("tp", "ep"),
            P("tp", "ep"),
            P("ep", "tp"),
            P("ep", None, "tp"),
            P("ep", None, "tp"),
            P("ep", "tp", None),
            P("ep", None),
            P("ep", None),
        ),
        out_specs=(P("ep", "tp"), P("ep", "tp", None, None)),
        check_vma=False,
    )
```

```python
import functools

import jax
import jax.numpy as jnp
from jax import lax
from jax.experimental import pallas as pl
from jax.experimental.pallas import tpu as pltpu
from jax.sharding import PartitionSpec as P

EXPERTS = 8
CAP = 5
SLOT = 8
SIDE = 4
PLANE = SIDE * SIDE
NEAR = (0, 1, 7, 2, 6, 3, 5, 4)
TRIPS = (
    ((1, 0, CAP), (2, 0, CAP), (6, 0, CAP), (7, 0, 1)),
    ((3, 0, CAP), (4, 0, CAP), (5, 0, CAP), (7, 1, 1)),
    ((7, 2, CAP - 2), (0, 0, CAP)),
)
CHUNKS = (16, 16, 8, 16)
DENSE = len(CHUNKS) - 1
GROUPS = 36
SENDS = 24
LOADS = 17
epsilon = 1e-06
MESH = pl.DeviceIdType.MESH
F32 = jnp.float32
BF16 = jnp.bfloat16


def dot(a, b):
    return jnp.dot(a, b, preferred_element_type=F32)


def dot_t(a, b):
    return lax.dot_general(a, b, (((1,), (1,)), ((), ())), preferred_element_type=F32)


def silu(v):
    return v / (1.0 + jnp.exp(-v))


def iota(shape, dim):
    return lax.broadcasted_iota(jnp.int32, shape, dim)


def kernel(
    tokens_h,
    norm_mix_h,
    routes_h,
    route_w_h,
    norm_ffn_h,
    gate_vec_h,
    state,
    w_query,
    w_key,
    w_value,
    w_out,
    dense_gate,
    dense_up,
    dense_down,
    exp_gate,
    exp_up,
    exp_down,
    mixed,
    ns,
    tokens,
    norm_mix,
    routes,
    route_w,
    norm_ffn,
    gate_vec,
    tok_p,
    wq,
    wk,
    wv,
    wo_o,
    wo_p,
    we,
    st,
    ho_o,
    ho_p,
    sel_m,
    scl_m,
    lg_s,
    lg_r,
    wbuf,
    w1,
    w2,
    w1d,
    w2d,
    xs,
    zr,
    xe_a,
    xe_b,
    xe_c,
    xe_d,
    pe_o_a,
    pe_o_b,
    pe_o_c,
    pe_o_d,
    pe_s_a,
    pe_s_b,
    pe_s_c,
    pe_s_d,
    pe_r_a,
    pe_r_b,
    pe_r_c,
    pe_r_d,
    y_a,
    y_b,
    y_c,
    y_d,
    yb_a,
    yb_b,
    yb_c,
    yb_d,
    rb_a,
    rb_b,
    rb_c,
    rb_d,
    sb_a,
    sb_b,
    sb_c,
    sb_d,
    ra_a,
    ra_b,
    ra_c,
    ra_d,
    tot,
    zs,
    zret,
    lsem,
    ssem,
    rsem,
    gsem,
):
    R, H = tokens.shape
    D = 2 * H
    heads, hs = state.shape[1], state.shape[2]
    HW = heads * hs
    FE = we.shape[2]
    FD = wbuf.shape[2]
    Z = EXPERTS
    me = lax.axis_index("ep")
    tp = lax.axis_index("tp")
    other = 1 - tp
    z, y_at, x_at = me // PLANE, (me // SIDE) % SIDE, me % SIDE

    def in_plane(dy, dx):
        return {
            "ep": z * PLANE + ((y_at + dy + SIDE) % SIDE) * SIDE + (x_at + dx + SIDE) % SIDE,
            "tp": tp,
        }

    first = {d: in_plane(tp * d, other * d) for d in (1, -1, 2)}
    second = {d: in_plane(other * d, tp * d) for d in (1, -1, 2)}
    zpeer = [{"ep": ((z + i) % Z) * PLANE + me % PLANE, "tp": tp} for i in range(Z)]
    partner = {"ep": me, "tp": other}

    own = pl.ds(pl.multiple_of(tp * H, H), H)
    oth = pl.ds(pl.multiple_of(other * H, H), H)

    sent, groups = [], []

    class Group:
        def __init__(self, whole, out=None):
            self.whole = whole
            self.k = groups.append(self) or len(groups) - 1
            self.out = sent.append(self) or len(sent) - 1 if out is None else out.out

        def copy(self, src, dst, dev):
            self.dev = dev
            return pltpu.make_async_remote_copy(
                src_ref=src,
                dst_ref=dst,
                send_sem=ssem.at[self.out],
                recv_sem=rsem.at[self.k],
                device_id=dev,
                device_id_type=MESH,
            )

        def add(self, src, dst, dev):
            self.copy(src, dst, dev).start()

        def wait_recv(self):
            self.copy(self.whole, self.whole, self.dev).wait_recv()

        def wait_send(self):
            self.copy(self.whole, self.whole, self.dev).wait_send()

    class Sends:
        def __init__(self, whole, dev):
            self.whole, self.dev = whole, dev
            self.out = sent.append(self) or len(sent) - 1

        def wait_send(self):
            pltpu.make_async_remote_copy(
                src_ref=self.whole,
                dst_ref=self.whole,
                send_sem=ssem.at[self.out],
                recv_sem=rsem.at[0],
                device_id=self.dev,
                device_id_type=MESH,
            ).wait_send()

    def remote(src, dst, dev):
        group = Group(dst)
        group.add(src, dst, dev)
        return group

    local = {}

    def load(name, src, dst):
        copy = pltpu.make_async_copy(src, dst, lsem.at[len(local)])
        copy.start()
        local[name] = copy

    HOPS = ((2, 3), (1, 1), (-1, 2))
    BACK = ((2, 3), (-1, 1), (1, 2))

    class Gather:
        def __init__(self, buf):
            self.at = buf.at

        def spread(self, *todo):
            for d, b in HOPS:
                for a in todo:
                    self.across.add(self.at[a], self.at[SIDE * b + a], second[d])

        def start(self):
            at = self.at
            out = Sends(at[pl.ds(1, PLANE - 1)], partner)
            self.near, self.far = Group(at[pl.ds(1, 2)], out), Group(at[3], out)
            self.across = Group(at[pl.ds(SIDE, 3 * SIDE)], out)
            self.far.add(at[0], at[3], first[2])
            self.near.add(at[0], at[1], first[1])
            self.near.add(at[0], at[2], first[-1])

        def go(self):
            self.near.wait_recv()
            self.spread(1, 2)
            self.far.wait_recv()
            self.spread(3)

    class Ring:
        def __init__(self, buf):
            self.at, self.step = buf.at, 0
            self.out = Sends(buf.at[pl.ds(1, Z - 1)], partner)

        def start(self):
            at, t = self.at, self.step
            if t:
                self.group.wait_recv()
            up, down = max(0, 2 * t), max(0, 2 * t - 1)
            if t < 3:
                self.group = Group(at[pl.ds(2 * t + 1, 2)], self.out)
                self.group.add(at[up], at[2 * t + 2], zpeer[1])
                self.group.add(at[down], at[2 * t + 1], zpeer[-1])
            elif t == 3:
                self.group = Group(at[7], self.out)
                self.group.add(at[up, pl.ds(0, 2)], at[7, pl.ds(0, 2)], zpeer[1])
                self.group.add(at[down, pl.ds(2, 1)], at[7, pl.ds(2, 1)], zpeer[-1])
            self.step = t + 1

    small = (
        (tokens_h, tokens),
        (norm_mix_h, norm_mix),
        (routes_h, routes),
        (route_w_h, route_w),
        (norm_ffn_h, norm_ffn),
        (gate_vec_h, gate_vec),
    )
    barrier = pltpu.get_barrier_semaphore()
    greeted = [partner, first[1], first[-1], second[1], second[-1], zpeer[1], zpeer[-1]]
    load("s0", tokens_h, tokens)
    for dev in greeted:
        pl.semaphore_signal(barrier, inc=1, device_id=dev, device_id_type=MESH)

    for t, (src, dst) in enumerate(small):
        if t:
            load(f"s{t}", src, dst)
    for t, src in enumerate((dense_gate, dense_up, dense_down)):
        load(f"d{t}", src, wbuf.at[0, t])
    for t, (src, dst) in enumerate(((w_query, wq), (w_key, wk), (w_value, wv))):
        load(f"p{t}", src, dst)
    load("st", state, st)
    load("wo", w_out, wo_o)
    load("eg", exp_gate.at[:, own], we.at[tp, 0])
    load("eu", exp_up.at[:, own], we.at[tp, 1])
    load("ed", exp_down.at[0, :, own], we.at[tp, 2])

    local["s0"].wait()
    pl.semaphore_wait(barrier, len(greeted))

    def tell(k, *devs):
        for dev in devs:
            pl.semaphore_signal(gsem.at[k], inc=1, device_id=dev, device_id_type=MESH)

    tell(0, first[-1])
    tell(1, second[-1])
    tell(2, zpeer[1], zpeer[-1])

    c_tok = remote(tokens, tok_p, partner)
    weights = Ring(wbuf)
    for t in range(3):
        local[f"d{t}"].wait()
    weights.start()
    c_wo = Group(wo_p)
    c_wo.add(w_out.at[:, oth], wo_p.at[0], partner)
    c_wo.add(w_out.at[:, own], wo_p.at[1], partner)
    c_we = Group(we.at[tp])
    for t, src in enumerate((exp_gate.at[:, oth], exp_up.at[:, oth], exp_down.at[0, :, oth])):
        c_we.add(src, we.at[tp, t], partner)

    for t in (2, 3):
        local[f"s{t}"].wait()
    row_id = iota((EXPERTS, R), 0)
    wt = jnp.zeros((EXPERTS, R), F32)
    member = jnp.zeros((EXPERTS, R), F32)
    named = routes[...]
    gains = route_w[...].astype(F32)
    for t in range(routes.shape[0]):
        hit = row_id == named[t : t + 1, :]
        wt = wt + jnp.where(hit, gains[t : t + 1, :], 0.0)
        member = member + jnp.where(hit, 1.0, 0.0)
    blank = jnp.zeros((EXPERTS, 128 - R), F32)
    wt = jnp.concatenate([wt, blank], axis=1)
    member = jnp.concatenate([member, blank], axis=1)
    before = jnp.where(iota((128, 128), 0) < iota((128, 128), 1), 1.0, 0.0).astype(BF16)
    rank = dot(member.astype(BF16), before)
    slot_id = iota((SLOT, 128), 0).astype(F32)
    picks = []
    for e in range(EXPERTS):
        pick = jnp.where(rank[e : e + 1] == slot_id, member[e : e + 1], 0.0)
        picks.append(pick)
        scl_m[e] = pick * wt[e : e + 1]
    sel_m[...] = jnp.concatenate(picks, axis=0)
    for t in (1, 4, 5):
        local[f"s{t}"].wait()

    tok_f = tokens[...].astype(F32)
    c_tok.wait_recv()
    tok_pf = tok_p[...].astype(F32)
    total = jnp.sum(tok_f * tok_f, axis=1, keepdims=True) + jnp.sum(
        tok_pf * tok_pf, axis=1, keepdims=True
    )
    scale = lax.rsqrt(total / D + epsilon)
    gain_o = norm_mix[:, own]
    gain_p = norm_mix[:, oth]
    nx_o = (tok_f * scale * gain_o).astype(BF16)
    nx_p = (tok_pf * scale * gain_p).astype(BF16)

    def project(w):
        return (dot(nx_o, w[own, :]) + dot(nx_p, w[oth, :])).astype(BF16).astype(F32)

    local["p0"].wait()
    q = project(wq)
    pad = jnp.zeros((128 - R, HW), F32)
    q_t = jnp.concatenate([q, pad], axis=0).T
    pl.semaphore_wait(gsem.at[2], 2)
    tell(3, zpeer[2], zpeer[-2])
    for t in (1, 2):
        local[f"p{t}"].wait()
    local["st"].wait()
    k = project(wk) * hs ** (-0.5)
    v = project(wv)
    k_t = jnp.concatenate([k, pad], axis=0).T
    head_id = tp * heads
    decays = []
    for h in range(heads):
        cols = slice(h * hs, (h + 1) * hs)
        idv = jnp.zeros((1, 128), F32) + (head_id + h).astype(F32)
        decay = 1.0 - jnp.exp2(-3.0 - 2.0 * idv)
        decays.append(decay)
        rows = []
        for s in range(R):
            rows.append(jnp.sum(st[s, h] * q_t[cols, s : s + 1], axis=0, keepdims=True))
        qs = jnp.concatenate(rows, axis=0)
        qk = jnp.sum(q[:, cols] * k[:, cols], axis=1, keepdims=True)
        read = decay * qs + qk * v[:, cols]
        centre = jnp.mean(read, axis=1, keepdims=True)
        dev = read - centre
        spread = jnp.mean(dev * dev, axis=1, keepdims=True)
        ho_o[:, cols] = (dev * lax.rsqrt(spread + epsilon)).astype(BF16)
    c_ho = remote(ho_o, ho_p, partner)
    ho = ho_o[...]
    local["wo"].wait()
    a_o = dot(ho, wo_o[:, own]).astype(BF16).astype(F32)
    a_p = dot(ho, wo_o[:, oth]).astype(BF16).astype(F32)
    c_wo.wait_recv()
    c_ho.wait_recv()
    hp = ho_p[...]
    a_o = a_o + dot(hp, wo_p[0]).astype(BF16).astype(F32)
    a_p = a_p + dot(hp, wo_p[1]).astype(BF16).astype(F32)
    after = (tok_f + a_o).astype(BF16).astype(F32)
    after_p = (tok_pf + a_p).astype(BF16).astype(F32)
    squares = jnp.sum(after * after, axis=1, keepdims=True) + jnp.sum(
        after_p * after_p, axis=1, keepdims=True
    )
    normed = (after * lax.rsqrt(squares / D + epsilon) * norm_ffn[...]).astype(BF16)

    pl.semaphore_wait(gsem.at[0], 1)
    pl.semaphore_wait(gsem.at[1], 1)
    pl.semaphore_wait(gsem.at[3], 2)
    chosen = dot(sel_m[:, :R].astype(BF16), normed).astype(BF16)
    xs[...] = chosen.astype(F32).reshape(EXPERTS, SLOT, H).astype(BF16)
    xe_d[0] = normed
    seat = {i: j for j, i in enumerate(NEAR)}
    z_out = Sends(zr.at[pl.ds(1, Z - 1)], partner)
    z_near, z_far = Group(zr.at[pl.ds(1, 4)], z_out), Group(zr.at[pl.ds(5, 3)], z_out)
    for i in (2, 6, 1, 7, 4, 3, 5):
        group = z_near if i in NEAR[:5] else z_far
        group.add(xs.at[(z + i) % Z], zr.at[seat[Z - i]], zpeer[i])
    xe = (xe_a, xe_b, xe_c, xe_d)
    chunks = [Gather(buf) for buf in xe]
    chunks[DENSE].start()
    chunks[DENSE].spread(0)
    gate_row = gate_vec[...].astype(F32)
    gate_row = jnp.concatenate([gate_row[r : r + 1] for r in range(H // 128)], axis=1)
    logit = jnp.sum(normed.astype(F32) * gate_row, axis=1, keepdims=True)
    lg_s[...] = logit + jnp.zeros((R, 128), F32)
    c_lg = remote(lg_s, lg_r, partner)
    def new_state(h):
        cols = slice(h * hs, (h + 1) * hs)
        for s in range(R):
            ns[s, h] = decays[h] * st[s, h] + k_t[cols, s : s + 1] * v[s : s + 1, cols]

    new_state(0)

    for name in ("eg", "eu", "ed"):
        local[name].wait()
    c_we.wait_recv()
    for t in range(2):
        for n, dst in enumerate((w1.at[0, t], w1.at[1, t], w2.at[t])):
            dst[:FE] = we[t, n]
            dst[FE:] = jnp.zeros((128 - FE, H), BF16)
    new_state(1)
    comb = [scl_m[(z + i) % Z] for i in NEAR]
    comb.append(jnp.zeros((128 - EXPERTS * SLOT, 128), F32))
    comb = jnp.concatenate(comb, axis=0).T[:R, : EXPERTS * SLOT].astype(BF16)

    pe_o = (pe_o_a, pe_o_b, pe_o_c, pe_o_d)
    pe_s = (pe_s_a, pe_s_b, pe_s_c, pe_s_d)
    pe_r = (pe_r_a, pe_r_b, pe_r_c, pe_r_d)
    y32, yb = (y_a, y_b, y_c, y_d), (yb_a, yb_b, yb_c, yb_d)
    rb, sb = (rb_a, rb_b, rb_c, rb_d), (sb_a, sb_b, sb_c, sb_d)
    ra = (ra_a, ra_b, ra_c, ra_d)
    enter = (w1, w1, w1, w1d)
    leave = (w2, w2, w2, w2d)

    def matches(shape, row_dim, order, trips):
        row, slot = iota(shape, row_dim), iota(shape, 1 - row_dim)
        found, first_row = jnp.zeros(shape, F32), 0
        for i, first_slot, count in trips:
            if i in order:
                shift = SLOT * order.index(i) + first_slot - first_row
                hit = (slot - row == shift) & (row >= first_row) & (row < first_row + count)
                found = found + jnp.where(hit, 1.0, 0.0)
            first_row += count
        return found.astype(BF16)

    def pack(c):
        order = [i for i, _, _ in TRIPS[c]]
        parts = [(zr[seat[i]] if i else xs[z]).astype(F32) for i in order]
        if len(parts) % 2:
            parts.append(jnp.zeros((SLOT, H), F32))
        rows = jnp.concatenate(parts, axis=0).astype(BF16)
        take = matches((CHUNKS[c], SLOT * len(parts)), 0, order, TRIPS[c])
        xe[c][0] = dot(take, rows).astype(BF16)
        chunks[c].start()

    z_near.wait_recv()
    pack(0)
    pack(2)
    chunks[0].spread(0)
    chunks[2].spread(0)
    weights.start()
    z_far.wait_recv()
    pack(1)
    chunks[1].spread(0)
    chunks[0].go()
    chunks[2].go()
    weights.start()
    chunks[1].go()
    chunks[DENSE].go()

    c_pe, c_rb, c_ra = {}, {}, {}

    def before_act(c):
        n = CHUNKS[c]
        chunks[c].across.wait_recv()
        x = xe[c][...].reshape(PLANE * n, H)
        weights_in = enter[c][...].reshape(512, H)
        c_pe[c] = Group(pe_r[c])
        for half in (slice(0, 256), slice(256, 512)):
            pre = dot_t(x, weights_in[half])
            pe_o[c][:, half] = pre
            for b in range(SIDE):
                for a in range(SIDE):
                    f = SIDE * b + a
                    pe_s[c][SIDE * a + b, :, half] = pre[f * n : (f + 1) * n].astype(BF16)
            lanes = pl.ds(half.start, 256)
            c_pe[c].add(pe_s[c].at[:, :, lanes], pe_r[c].at[:, :, lanes], partner)

    def act(c):
        n = CHUNKS[c]
        c_pe[c].wait_recv()
        pre = pe_o[c][...] + pe_r[c][...].astype(F32).reshape(PLANE * n, 512)
        hidden = (silu(pre[:, :256]) * pre[:, 256:]).astype(BF16)
        down = leave[c][...].reshape(256, H)
        gone = dot(hidden[SIDE * n :], down)
        yb[c][...] = gone.reshape(3 * SIDE, n, H).astype(BF16)
        out, at = yb[c].at, rb[c].at
        c_rb[c] = Group(rb[c])
        for d, b in BACK:
            c_rb[c].add(out[pl.ds(SIDE * (b - 1), SIDE)], at[b - 1], second[d])
        y32[c][...] = dot(hidden[: SIDE * n], down).reshape(SIDE, n, H)

    def sum_second(c):
        c_rb[c].wait_recv()
        total = y32[c][...]
        for b in range(3):
            total = total + rb[c][b].astype(F32)
        sb[c][...] = total[1:].astype(BF16)
        c_ra[c] = Group(ra[c])
        for d, a in BACK:
            c_ra[c].add(sb[c].at[a - 1], ra[c].at[a - 1], first[d])
        y32[c][0] = total[0]

    c_ret = Group(zret.at[pl.ds(1, Z - 1)])

    def sum_first(c):
        c_ra[c].wait_recv()
        total = y32[c][0]
        for a in range(3):
            total = total + ra[c][a].astype(F32)
        return total

    def give_back(c, *order):
        tot[sum(CHUNKS[:c]) : sum(CHUNKS[: c + 1])] = sum_first(c)
        done = tot[: sum(CHUNKS[: c + 1])]
        pad = -done.shape[0] % 16
        if pad:
            done = jnp.concatenate([done, jnp.zeros((pad, H), F32)], axis=0)
        put = matches((SLOT * len(order), done.shape[0]), 1, order, sum(TRIPS[: c + 1], ()))
        rows = dot(put, done.astype(BF16))
        for n, i in enumerate(order):
            block = rows[n * SLOT : (n + 1) * SLOT].astype(BF16)
            if i == 0:
                zret[0] = block
            else:
                zs[i] = block
                c_ret.add(zs.at[i], zret.at[seat[Z - i]], zpeer[i])

    before_act(0)
    weights.start()
    act(0)
    before_act(1)
    before_act(2)
    act(1)
    weights.start()
    for j in range(Z):
        for t, dst in enumerate((w1d.at[0, j], w1d.at[1, j], w2d.at[j])):
            dst[:FD] = wbuf[j, t]
            dst[FD:] = jnp.zeros((32 - FD, H), BF16)
    before_act(DENSE)
    act(2)
    act(DENSE)
    sum_second(0)
    sum_second(1)
    give_back(0, 1, 2, 6)
    sum_second(2)
    give_back(1, 3, 4, 5)
    sum_second(DENSE)
    give_back(2, 7, 0)
    dense = sum_first(DENSE)

    c_lg.wait_recv()
    open_ = 1.0 / (1.0 + jnp.exp(-(lg_s[:, :1] + lg_r[:, :1])))
    c_ret.wait_recv()
    back = zret[...].astype(F32).reshape(EXPERTS * SLOT, H).astype(BF16)
    moe = dot(comb, back)
    mixed[...] = (after + moe + open_ * dense).astype(BF16)
    for group in sent:
        group.wait_send()
    assert (len(groups), len(sent), len(local)) == (GROUPS, SENDS, LOADS), (len(groups), len(sent))


def store(a_in, b_in, a_out, b_out, sems):
    first = pltpu.make_async_copy(b_in, b_out, sems.at[0])
    second = pltpu.make_async_copy(a_in, a_out, sems.at[1])
    first.start()
    second.start()
    first.wait()
    second.wait()


def body(
    tokens,
    state,
    norm_mix,
    w_query,
    w_key,
    w_value,
    w_out,
    norm_ffn,
    gate_vector,
    dense_gate,
    dense_up,
    dense_down,
    exp_gate,
    exp_up,
    exp_down,
    routes,
    route_w,
):
    R, H = tokens.shape
    heads, hs = state.shape[1], state.shape[2]
    HW = heads * hs
    FE = exp_gate.shape[2]
    FD = dense_gate.shape[1]
    Z = EXPERTS
    per_chunk = lambda make: [make(n) for n in CHUNKS]
    vm = pl.BlockSpec(memory_space=pltpu.VMEM)
    hbm = pl.BlockSpec(memory_space=pltpu.HBM)
    V = pltpu.VMEM
    sem = lambda *shape: pltpu.SemaphoreType.DMA(shape)
    operands = (
        tokens,
        norm_mix.reshape(1, -1),
        routes.T,
        route_w.T,
        norm_ffn.reshape(1, -1),
        gate_vector.reshape(-1, 128),
        state,
        w_query,
        w_key,
        w_value,
        w_out,
        dense_gate.T,
        dense_up.T,
        dense_down,
        exp_gate[0].T,
        exp_up[0].T,
        exp_down,
    )
    held = [pltpu.with_memory_space_constraint(x, pltpu.HBM) for x in operands]
    mixed, new_state = pl.pallas_call(
        kernel,
        out_shape=(pltpu.VMEM((R, H), BF16), pltpu.VMEM(state.shape, F32)),
        in_specs=[hbm] * 17,
        out_specs=(vm, vm),
        scratch_shapes=[
            V((R, H), BF16),
            V((1, 2 * H), F32),
            V((routes.shape[1], R), jnp.int32),
            V((routes.shape[1], R), BF16),
            V((1, H), F32),
            V((H // 128, 128), BF16),
            V((R, H), BF16),
            V((2 * H, HW), BF16),
            V((2 * H, HW), BF16),
            V((2 * H, HW), BF16),
            V((HW, 2 * H), BF16),
            V((2, HW, H), BF16),
            V((2, 3, FE, H), BF16),
            V(state.shape, F32),
            V((R, HW), BF16),
            V((R, HW), BF16),
            V((EXPERTS * SLOT, 128), F32),
            V((EXPERTS, SLOT, 128), F32),
            V((R, 128), F32),
            V((R, 128), F32),
            V((Z, 3, FD, H), BF16),
            V((2, 2, 128, H), BF16),
            V((2, 128, H), BF16),
            V((2, Z, 32, H), BF16),
            V((Z, 32, H), BF16),
            V((EXPERTS, SLOT, H), BF16),
            V((Z, SLOT, H), BF16),
            *per_chunk(lambda n: V((PLANE, n, H), BF16)),
            *per_chunk(lambda n: V((PLANE * n, 512), F32)),
            *per_chunk(lambda n: V((PLANE, n, 512), BF16)),
            *per_chunk(lambda n: V((PLANE, n, 512), BF16)),
            *per_chunk(lambda n: V((SIDE, n, H), F32)),
            *per_chunk(lambda n: V((3 * SIDE, n, H), BF16)),
            *per_chunk(lambda n: V((3, SIDE, n, H), BF16)),
            *per_chunk(lambda n: V((3, n, H), BF16)),
            *per_chunk(lambda n: V((3, n, H), BF16)),
            V((sum(CHUNKS[:DENSE]), H), F32),
            V((Z, SLOT, H), BF16),
            V((Z, SLOT, H), BF16),
            sem(LOADS),
            sem(SENDS),
            sem(GROUPS),
            pltpu.SemaphoreType.REGULAR((4,)),
        ],
        compiler_params=pltpu.CompilerParams(
            collective_id=0, has_side_effects=True, vmem_limit_bytes=50 * 1024 * 1024
        ),
        name="layer",
    )(
        *held
    )
    return pl.pallas_call(
        store,
        out_shape=(
            jax.ShapeDtypeStruct((R, H), BF16),
            jax.ShapeDtypeStruct(state.shape, F32),
        ),
        in_specs=[vm, vm],
        out_specs=(hbm, hbm),
        scratch_shapes=[sem(2)],
        name="store",
    )(
        pltpu.with_memory_space_constraint(mixed, pltpu.VMEM),
        pltpu.with_memory_space_constraint(new_state, pltpu.VMEM),
    )


def solution(mesh):
    return jax.shard_map(
        body,
        mesh=mesh,
        in_specs=(
            P("ep", "tp"),
            P("ep", "tp", None, None),
            P(),
            P(None, "tp"),
            P(None, "tp"),
            P(None, "tp"),
            P("tp", None),
            P("tp"),
            P("tp"),
            P("tp", "ep"),
            P("tp", "ep"),
            P("ep", "tp"),
            P("ep", None, "tp"),
            P("ep", None, "tp"),
            P("ep", "tp", None),
            P("ep", None),
            P("ep", None),
        ),
        out_specs=(P("ep", "tp"), P("ep", "tp", None, None)),
        check_vma=False,
    )
```
